32 devices in a mesh: sp: 16 (over z, y, x), tp: 2 (over core).
Axes of the slice: x: 2, y: 2, z: 4, core: 2. Of those that a mesh axis runs over, the one named last changes fastest.
Arguments:
- conv_value: bfloat16 [4096, 1024], P('sp', 'tp'), may hold values from -6 to 6
- conv_gate: bfloat16 [4096, 1024], P('sp', 'tp'), may hold values from -6 to 6
- taps: bfloat16 [31, 1024], P(None, 'tp'), may hold values from -1 to 1
- doc_ids: int32 [4096], P('sp'), may hold values from 0 to 3, never falling along the last dimension, each value on 1 to 2048 neighbouring positions
- gn_gain: float32 [1024], P('tp'), may hold values from 0.1 to 1.9
- gn_shift: float32 [1024], P('tp'), may hold values from -3 to 3
- conv_out: bfloat16 [1024, 2048], replicated, may hold values from -0.1875 to 0.1875
- residual: bfloat16 [4096, 2048], P(('sp', 'tp')), may hold values from -6 to 6
- norm_gain: float32 [2048], replicated, may hold values from 0.1 to 1.9
- routes: int32 [4096, 2], P(('sp', 'tp')), may hold values from 0 to 31, as said below
- route_weight: float32 [4096, 2], P(('sp', 'tp')), may hold values from 0.3 to 1.2
- expert_gate: bfloat16 [32, 2048, 512], P(('sp', 'tp')), may hold values from -0.125 to 0.125
- expert_up: bfloat16 [32, 2048, 512], P(('sp', 'tp')), may hold values from -0.125 to 0.125
- expert_down: bfloat16 [32, 512, 2048], P(('sp', 'tp')), may hold values from -0.25 to 0.25
- shared_gate: bfloat16 [2048, 512], replicated, may hold values from -0.125 to 0.125
- shared_up: bfloat16 [2048, 512], replicated, may hold values from -0.125 to 0.125
- shared_down: bfloat16 [512, 2048], replicated, may hold values from -0.25 to 0.25
Outputs:
- layer_out: bfloat16 [4096, 2048], P(('sp', 'tp'))
The draws below stay inside these ranges and needn't reach their ends.
Inputs may be any that keep to these rules, and one draw needn't show every extreme that they name: `routes`: each row names 2 different experts. The rows of one device name each expert at most 16 times, and one expert, the same for every device, exactly 16 times. `doc_ids`: numbers never fall from one position to the next.
All inputs are finite; a program needn't handle non-finite values.
Results may differ from the reference program's by a relative error of at most 0.014.
Values may be sent and summed in bfloat16 or wider, within the bound.
A program may use at most 128 MiB of HBM per device.

```python
import math
import jax
import jax.numpy as jnp
import numpy as np
from jax import lax

D = 2048
CONV_DIM = 1024
GROUPS = 8
WIDTH = 31
EXPERT_DIM = 512
SHARED_DIM = 512
TOP_K = 2
TOK_SP = 256
TOK_DEV = 128
TOKENS = 4096
EXPERTS = 32
CAP = 16
DOCS = 4


def draw_routes(key, part):
    blocks = TOKENS // TOK_DEV
    pairs = EXPERTS // 2
    key_order = jax.random.fold_in(key, 11)
    key_tilt = jax.random.fold_in(key, 12)
    key_noise = jax.random.fold_in(key, 13)
    key_rows = jax.random.fold_in(key, 14)
    order = jax.random.permutation(key_order, EXPERTS).astype(jnp.int32)
    tilt = jax.random.randint(key_tilt, (pairs,), 0, CAP + 1)
    noise = jax.random.randint(key_noise, (blocks, pairs), -(CAP // 4), CAP // 4 + 1)
    first = jnp.clip(tilt[None, :] + noise, 0, CAP)
    first = first.at[:, 0].set(CAP)
    pair_counts = jnp.stack([first, CAP - first], axis=2).reshape(blocks, EXPERTS)
    counts = jnp.zeros((blocks, EXPERTS), jnp.int32).at[:, order].set(pair_counts.astype(jnp.int32))
    cumulative = jnp.cumsum(counts, axis=1).astype(jnp.int32)
    positions = jnp.arange(TOK_DEV * TOP_K, dtype=jnp.int32)
    expert_of = jax.vmap(lambda row: jnp.searchsorted(row, positions, side='right'))(cumulative).astype(jnp.int32)
    slots = expert_of.reshape(blocks, TOP_K, TOK_DEV).transpose(0, 2, 1)
    row_keys = jax.random.split(key_rows, blocks)
    shuffles = jax.vmap(lambda one_key: jax.random.permutation(one_key, TOK_DEV))(row_keys).astype(jnp.int32)
    shuffles = jnp.broadcast_to(shuffles[:, :, None], (blocks, TOK_DEV, TOP_K))
    shuffled = jnp.take_along_axis(slots, shuffles, axis=1)
    return shuffled.reshape(TOKENS, TOP_K).astype(jnp.int32)


def level_of(key, extent, shards, low, high):
    loudness = 1.0
    for dim, parts in shards:
        draws = jax.random.uniform(jax.random.fold_in(jax.random.fold_in(key, 6), dim), (parts,), jnp.float32, low / len(shards), high / len(shards))
        loudness = loudness * jnp.repeat(jnp.exp(draws), extent[dim] // parts).reshape((-1,) + (1,) * (len(extent) - 1 - dim))
    return loudness


def length_profile(count, total, reach, slope):
    weights = [(1 << 20) // math.isqrt(rank ** slope) + 1 for rank in range(2, count + 1)]
    rest, holding = total - reach - (count - 1), [1] * (count - 1)
    while rest > 0:
        candidates = [i for i in range(count - 1) if holding[i] < reach]
        pool, left = sum([weights[i] for i in candidates]), rest
        for i in candidates:
            more = min(reach - holding[i], max(1, left * weights[i] // pool), rest)
            holding[i] = holding[i] + more
            rest = rest - more
    return np.array([reach] + holding)


def uneven_parts(own_key, amount, total, bound, lean):
    if amount == 2:
        one = jax.random.randint(own_key, (), max(1, total - bound), min(bound, total - 1) + 1)
        return jnp.stack([one, total - one])
    sizes = jnp.asarray(length_profile(amount, total, bound, lean), jnp.int32)
    couples = (amount - 1) // 2
    giver, taker = sizes[1:1 + 2 * couples:2], sizes[2:2 + 2 * couples:2]
    room = jnp.minimum(giver - 1, bound - taker)
    moved = jax.random.randint(jax.random.fold_in(own_key, 1), (couples,), 0, 1 << 20) % (room + 1)
    sizes = sizes.at[1:1 + 2 * couples:2].set(giver - moved).at[2:2 + 2 * couples:2].set(taker + moved)
    return sizes[jax.random.permutation(jax.random.fold_in(own_key, 2), amount)]


def normal_values(own_key, dims, scale, most, cuts=(), kind=jnp.bfloat16):
    array = scale * jax.random.normal(own_key, dims, jnp.float32)
    if cuts:
        array = array * level_of(own_key, dims, cuts, -0.22, 0.18)
    return jnp.clip(array, -most, most).astype(kind)


def setup_inputs(seed: int = 0) -> dict:
    arg_keys = jax.random.split(jax.random.key(seed), 18)
    return {
        "conv_value": normal_values(arg_keys[0], (TOKENS, CONV_DIM), 1.0, 6.0, ((0, 16), (1, 2))),
        "conv_gate": normal_values(arg_keys[1], (TOKENS, CONV_DIM), 1.0, 6.0, ((0, 16), (1, 2))),
        "taps": normal_values(arg_keys[2], (WIDTH, CONV_DIM), WIDTH ** -0.5, 1.0, ((1, 2),)),
        "doc_ids": jnp.searchsorted(jnp.cumsum(uneven_parts(arg_keys[3], DOCS, TOKENS, 8 * TOK_SP, 1)), jnp.arange(TOKENS), side="right").astype(jnp.int32),
        "gn_gain": jnp.clip(1.0 + 0.18 * jax.random.normal(arg_keys[4], (CONV_DIM,), jnp.float32), 0.1, 1.9),
        "gn_shift": normal_values(arg_keys[5], (CONV_DIM,), 0.5, 3.0, ((0, 2),), jnp.float32),
        "conv_out": normal_values(arg_keys[6], (CONV_DIM, D), CONV_DIM ** -0.5, 0.1875),
        "residual": normal_values(arg_keys[7], (TOKENS, D), 1.0, 6.0, ((0, 32),)),
        "norm_gain": jnp.clip(1.0 + 0.18 * jax.random.normal(arg_keys[8], (D,), jnp.float32), 0.1, 1.9),
        "routes": draw_routes(jax.random.fold_in(arg_keys[17], 71), 0),
        "route_weight": jnp.clip(0.3 + 0.90000004 * jax.random.uniform(arg_keys[10], (TOKENS, TOP_K), jnp.float32) ** level_of(arg_keys[10], (TOKENS, TOP_K), ((0, 32),), -0.2, 0.2), 0.3, 1.2),
        "expert_gate": normal_values(arg_keys[11], (EXPERTS, D, EXPERT_DIM), D ** -0.5, 0.125, ((0, 32),)),
        "expert_up": normal_values(arg_keys[12], (EXPERTS, D, EXPERT_DIM), D ** -0.5, 0.125, ((0, 32),)),
        "expert_down": normal_values(arg_keys[13], (EXPERTS, EXPERT_DIM, D), EXPERT_DIM ** -0.5, 0.25, ((0, 32),)),
        "shared_gate": normal_values(arg_keys[14], (D, SHARED_DIM), D ** -0.5, 0.125),
        "shared_up": normal_values(arg_keys[15], (D, SHARED_DIM), D ** -0.5, 0.125),
        "shared_down": normal_values(arg_keys[16], (SHARED_DIM, D), SHARED_DIM ** -0.5, 0.25),
    }


epsilon = 1e-06

def route_rows(normed, routes, route_weight, expert_gate, expert_up, expert_down):
    blocks = TOKENS // TOK_DEV
    flat_routes = routes.reshape(blocks, TOK_DEV * TOP_K).astype(jnp.int32)
    onehot = (flat_routes[:, :, None] == jnp.arange(EXPERTS, dtype=jnp.int32)[None, None, :]).astype(jnp.int32)
    slot_index = (lax.optimization_barrier(jnp.sum(jnp.cumsum(onehot, axis=1) * onehot, axis=2)) - 1).astype(jnp.int32)
    block_index = jnp.broadcast_to(jnp.arange(blocks, dtype=jnp.int32)[:, None], flat_routes.shape)
    row_index = (block_index * TOK_DEV + jnp.arange(TOK_DEV * TOP_K, dtype=jnp.int32)[None, :] // TOP_K).astype(jnp.int32)
    slot_table = jnp.full((EXPERTS, blocks, CAP), TOKENS, jnp.int32).at[flat_routes, block_index, slot_index].set(row_index)
    weight_table = jnp.zeros((EXPERTS, blocks, CAP), jnp.float32).at[flat_routes, block_index, slot_index].set(route_weight.reshape(blocks, TOK_DEV * TOP_K).astype(jnp.float32))
    padded_rows = jnp.concatenate([normed, jnp.zeros((1, D), normed.dtype)], axis=0)

    def one_expert(routed_sum, pieces):
        table_rows, table_weights, gate_weight, up_weight, down_weight = pieces
        expert_rows = padded_rows[table_rows]
        gate_part = jnp.dot(expert_rows, gate_weight, preferred_element_type=jnp.float32)
        up_part = jnp.dot(expert_rows, up_weight, preferred_element_type=jnp.float32)
        hidden = (jax.nn.silu(gate_part) * up_part).astype(jnp.bfloat16)
        result = jnp.dot(hidden, down_weight, preferred_element_type=jnp.float32).astype(jnp.bfloat16)
        routed_sum = routed_sum.at[table_rows].add(table_weights[:, None] * result.astype(jnp.float32), mode='drop')
        return (routed_sum, None)
    routed, _ = lax.scan(one_expert, jnp.zeros((TOKENS, D), jnp.float32), (slot_table.reshape(EXPERTS, blocks * CAP), weight_table.reshape(EXPERTS, blocks * CAP), expert_gate, expert_up, expert_down))
    return routed

def reference(conv_value, conv_gate, taps, doc_ids, gn_gain, gn_shift, conv_out, residual, norm_gain, routes, route_weight, expert_gate, expert_up, expert_down, shared_gate, shared_up, shared_down):
    glu = (conv_value.astype(jnp.float32) * jax.nn.sigmoid(conv_gate.astype(jnp.float32))).astype(jnp.bfloat16)
    padded_glu = jnp.pad(glu, ((WIDTH - 1, 0), (0, 0)))
    padded_ids = jnp.pad(doc_ids, (WIDTH - 1, 0), constant_values=-1)
    conv_sum = jnp.zeros((TOKENS, CONV_DIM), jnp.float32)
    for offset in range(WIDTH):
        same_doc = (padded_ids[offset:offset + TOKENS] == doc_ids)[:, None]
        tap_term = taps[offset].astype(jnp.float32)[None, :] * padded_glu[offset:offset + TOKENS].astype(jnp.float32)
        conv_sum = conv_sum + jnp.where(same_doc, tap_term, 0.0)
    grouped = conv_sum.reshape(TOKENS, GROUPS, CONV_DIM // GROUPS)
    group_mean = lax.optimization_barrier(jnp.mean(grouped, axis=-1, keepdims=True))
    centered = grouped - group_mean
    group_var = lax.optimization_barrier(jnp.mean(centered * centered, axis=-1, keepdims=True))
    normalized = (centered * lax.rsqrt(group_var + epsilon)).reshape(TOKENS, CONV_DIM)
    conv_act = jax.nn.silu(normalized * gn_gain + gn_shift).astype(jnp.bfloat16)
    projected = jnp.dot(conv_act, conv_out, preferred_element_type=jnp.float32)
    stream = (residual.astype(jnp.float32) + projected).astype(jnp.bfloat16)
    stream_wide = stream.astype(jnp.float32)
    normed = (stream_wide * lax.rsqrt(lax.optimization_barrier(jnp.mean(stream_wide * stream_wide, axis=-1, keepdims=True)) + epsilon) * norm_gain).astype(jnp.bfloat16)
    shared_hidden = (jax.nn.silu(jnp.dot(normed, shared_gate, preferred_element_type=jnp.float32)) * jnp.dot(normed, shared_up, preferred_element_type=jnp.float32)).astype(jnp.bfloat16)
    shared_out = jnp.dot(shared_hidden, shared_down, preferred_element_type=jnp.float32)
    routed = route_rows(normed, routes, route_weight, expert_gate, expert_up, expert_down)
    return (stream_wide + shared_out + routed).astype(jnp.bfloat16)
```

```python
import functools

import jax
import jax.numpy as jnp
from jax import lax
from jax.experimental import pallas as pl
from jax.experimental.pallas import tpu as pltpu
from jax.sharding import PartitionSpec as P

GROUPS = 8


epsilon = 1e-06


def from_behind(x, axis, by):
    peers = lax.axis_size(axis)
    pairs = [(i, i + by) for i in range(peers) if 0 <= i + by < peers]
    return lax.ppermute(x, axis, pairs)


def per_device(
    conv_value,
    conv_gate,
    taps,
    doc_ids,
    gn_gain,
    gn_shift,
    conv_out,
    residual,
    norm_gain,
    routes,
    route_weight,
    expert_gate,
    expert_up,
    expert_down,
    shared_gate,
    shared_up,
    shared_down,
):
    position_count, channel_count = conv_value.shape
    kernel_width = taps.shape[0]
    model_width = residual.shape[1]
    glu_out = (
        conv_value.astype(jnp.float32) * jax.nn.sigmoid(conv_gate.astype(jnp.float32))
    ).astype(jnp.bfloat16)
    rim_start = position_count - kernel_width + 1
    edge_glu, edge_ids = from_behind((glu_out[rim_start:], doc_ids[rim_start:]), "sp", 1)
    longer_glu = jnp.concatenate([edge_glu, glu_out], axis=0)
    longer_ids = jnp.concatenate([edge_ids, doc_ids], axis=0)
    conv_sum = jnp.zeros((position_count, channel_count), jnp.float32)
    for offset in range(kernel_width):
        same_doc = (longer_ids[offset : offset + position_count] == doc_ids)[:, None]
        tap_term = taps[offset].astype(jnp.float32)[None, :] * longer_glu[
            offset : offset + position_count
        ].astype(jnp.float32)
        conv_sum = conv_sum + jnp.where(same_doc, tap_term, 0.0)
    core_split = lax.axis_size("tp")
    groups_here = GROUPS // core_split
    grouped = conv_sum.reshape(position_count, groups_here, channel_count // groups_here)
    group_mean = jnp.mean(grouped, axis=-1, keepdims=True)
    centered = grouped - group_mean
    group_var = jnp.mean(centered * centered, axis=-1, keepdims=True)
    normalized = (centered * lax.rsqrt(group_var + epsilon)).reshape(position_count, channel_count)
    conv_act = jax.nn.silu(normalized * gn_gain + gn_shift).astype(jnp.bfloat16)
    token_rows = lax.all_to_all(conv_act, "tp", split_axis=0, concat_axis=1, tiled=True)
    projected = jnp.dot(token_rows, conv_out, preferred_element_type=jnp.float32)
    stream = (residual.astype(jnp.float32) + projected).astype(jnp.bfloat16)
    stream_wide = stream.astype(jnp.float32)
    normed = (
        stream_wide
        * lax.rsqrt(jnp.mean(stream_wide * stream_wide, axis=-1, keepdims=True) + epsilon)
        * norm_gain
    ).astype(jnp.bfloat16)
    token_count, top_count = routes.shape
    sequence_split = lax.axis_size("sp")
    device_count = sequence_split * core_split
    local_experts = expert_gate.shape[0]
    experts = local_experts * device_count
    capacity = 2 * token_count * top_count // experts
    flat_routes = routes.reshape(-1)
    onehot = (flat_routes[:, None] == jnp.arange(experts, dtype=jnp.int32)[None, :]).astype(
        jnp.int32
    )
    slot_index = jnp.sum(jnp.cumsum(onehot, axis=0) * onehot, axis=1) - 1
    target = flat_routes * capacity + slot_index
    source = (
        jnp.full((experts * capacity,), token_count, jnp.int32)
        .at[target]
        .set(jnp.arange(token_count * top_count, dtype=jnp.int32) // top_count)
    )
    padded_rows = jnp.concatenate([normed, jnp.zeros((1, model_width), normed.dtype)], axis=0)
    outgoing = padded_rows[source]
    shared_hidden = (
        jax.nn.silu(jnp.dot(normed, shared_gate, preferred_element_type=jnp.float32))
        * jnp.dot(normed, shared_up, preferred_element_type=jnp.float32)
    ).astype(jnp.bfloat16)
    shared_out = jnp.dot(shared_hidden, shared_down, preferred_element_type=jnp.float32)
    parcel = outgoing.reshape(device_count, local_experts, capacity, model_width)
    arrived = lax.all_to_all(parcel, ("sp", "tp"), split_axis=0, concat_axis=0, tiled=True)
    expert_rows = arrived[:, 0].reshape(-1, model_width)
    gate_part = jnp.dot(expert_rows, expert_gate[0], preferred_element_type=jnp.float32)
    up_part = jnp.dot(expert_rows, expert_up[0], preferred_element_type=jnp.float32)
    hidden = (jax.nn.silu(gate_part) * up_part).astype(jnp.bfloat16)
    result = jnp.dot(hidden, expert_down[0], preferred_element_type=jnp.float32).astype(
        jnp.bfloat16
    )
    results = [result.reshape(arrived.shape[0], arrived.shape[2], model_width)]
    returned = lax.all_to_all(
        jnp.stack(results, axis=1), ("sp", "tp"), split_axis=0, concat_axis=0, tiled=True
    )
    picked = returned.reshape(experts * capacity, model_width)[target].reshape(
        token_count, top_count, model_width
    )
    routed = jnp.zeros((token_count, model_width), jnp.float32)
    for route_index in range(top_count):
        routed = routed + route_weight[:, route_index, None] * picked[:, route_index].astype(
            jnp.float32
        )
    return (stream_wide + shared_out + routed).astype(jnp.bfloat16)


F32 = jnp.float32
BF16 = jnp.bfloat16
MESH_ID = pl.DeviceIdType.MESH
HALO = 32
CHUNK = 32
PLANES = 4
PARTS = 4
VMEM_LIMIT = 58 * 1024 * 1024


def flip(index, bits):
    out, weight = index, 1
    while weight <= bits:
        if (bits // weight) % 2:
            out = out + weight * (1 - 2 * ((index // weight) % 2))
        weight *= 2
    return out


def silu(v):
    return v / (1.0 + jnp.exp(-v))


ORDERS = {
    "E": (
        "P01", "D03", "D00", "P02", "P03", "T10", "S00", "P00", "P12", "T20", "P11", "D02",
        "D01", "T30", "X00", "P13", "P10", "P33", "P30", "X10", "P32", "M10", "P31", "P20",
        "M13", "P23", "X30", "M00", "M11", "M02", "M03", "P22", "M30", "P21", "M31", "M32",
        "X20", "M33", "M20", "M22", "M23", "M21", "F00", "M12", "M01", "F02", "F01", "F03",
    ),
    "I": (
        "D12", "D00", "D03", "P02", "D11", "P00", "D13", "R00", "T30", "L13", "L10", "D10",
        "P03", "T20", "L33", "P01", "L12", "P33", "L30", "L20", "D02", "T10", "X00", "L11",
        "P30", "P10", "D01", "L32", "L31", "P31", "P32", "L23", "P13", "L21", "P20", "P21",
        "P11", "S00", "P23", "P12", "L22", "P22", "X30", "M00", "X10", "M03", "M30", "M01",
        "M31", "M10", "M32", "X20", "M11", "M33", "M12", "M20", "M13", "M22", "M02", "M23",
        "M21", "F03", "F00", "F02", "F01",
    ),
}


def fused_kernel(n_sp, n_tp, capacity, *refs):
    hbm_in, out_hbm = refs[:17], refs[17]
    vmem_in = refs[18:35]
    (
        glu_ext,
        ids_ext,
        tap_rows,
        halo_send,
        halo_recv,
        act,
        act_recv,
        ids_here,
        base_ref,
        mail,
        picks,
        highs,
        lows,
        tok,
        outgoing,
        arrived,
        result,
        returned,
        partial,
        inc,
        out_ref,
        load_sem,
        halo_sem,
        act_sem,
        mail_send,
        mail_recv,
        tok_send,
        tok_recv,
        go_send,
        go_recv,
        back_send,
        back_recv,
        part_send,
        part_recv,
        out_sem,
    ) = refs[35:]
    (
        value_ref,
        gate_ref,
        taps_ref,
        ids_ref,
        gain_ref,
        shift_ref,
        resid_ref,
        ngain_ref,
        routes_ref,
        weight_ref,
        conv_out,
        sg,
        su,
        sd,
        eg,
        eu,
        ed,
    ) = vmem_in
    n = n_sp * n_tp
    per = n // PLANES
    sp, tp = lax.axis_index("sp"), lax.axis_index("tp")
    me = sp * n_tp + tp
    plane, here = me // per, me % per
    rows, channels = value_ref.shape
    tokens, model = resid_ref.shape
    width = taps_ref.shape[0]
    group = glu_ext.shape[2]
    groups = channels // group
    cols = model // PARTS
    slots = per * capacity
    side = 1 - 2 * (plane // 2)
    edge = plane % (PLANES - 1) == 0
    inner = plane % (PLANES - 1) != 0
    inner_count = (plane % (PLANES - 1) + 1) // 2

    def place(index):
        return (index // n_tp, index % n_tp)

    inward = place((plane + side) * per + here)
    outward = place((plane - side) * per + here)
    peers = [flip(here, k) for k in range(per - 1, 0, -1)]

    def peer_place(peer):
        return place(plane * per + peer)

    loads = [
        pltpu.make_async_copy(a, b, load_sem.at[i])
        for i, (a, b) in enumerate(zip(hbm_in, vmem_in))
    ]
    barrier = pltpu.get_barrier_semaphore()

    def greet(where):
        pl.semaphore_signal(barrier, inc=1, device_id=where, device_id_type=MESH_ID)

    for load in loads:
        load.start()
    for peer in peers:
        greet(peer_place(peer))
    greet(inward)

    @pl.when(inner)
    def _():
        greet(outward)

    @pl.when(sp < n_sp - 1)
    def _():
        greet((sp + 1, tp))

    @pl.when(sp > 0)
    def _():
        greet((sp - 1, tp))

    has_next = 1 - (sp + 1) // n_sp
    has_last = (sp + n_sp - 1) // n_sp
    for load in loads[:10]:
        load.wait()

    mail[0, 0:2, :] = routes_ref[...].astype(F32)
    mail[0, 2:4, :] = weight_ref[...]
    glu = (value_ref[...].astype(F32) * jax.nn.sigmoid(gate_ref[...].astype(F32))).astype(BF16)
    halo_send[...] = glu[rows - HALO :, :]
    for g in range(groups):
        glu_ext[g, pl.ds(HALO, rows), :] = glu[:, g * group : (g + 1) * group].astype(F32)
    for at in range(0, rows, group):
        row = ids_ref[:, at : at + group].astype(F32)
        column = jnp.broadcast_to(row, (group, group)).T
        ids_here[pl.ds(at, group), :] = column
        ids_ext[pl.ds(HALO + at, group), :] = column
    tap_rows[pl.ds(0, width), :] = taps_ref[...].astype(F32)

    def remote(src, dst, send_sem, recv_sem, where):
        return pltpu.make_async_remote_copy(
            src_ref=src,
            dst_ref=dst,
            send_sem=send_sem,
            recv_sem=recv_sem,
            device_id=where,
            device_id_type=MESH_ID,
        )

    halo_copies = [
        remote(halo_send, halo_recv, halo_sem.at[0], halo_sem.at[1], (sp + 1, tp)),
        remote(
            ids_here.at[pl.ds(rows - HALO, HALO)],
            ids_ext.at[pl.ds(0, HALO)],
            halo_sem.at[2],
            halo_sem.at[3],
            (sp + 1, tp),
        ),
    ]

    @pl.when(sp == 0)
    def _():
        glu_ext[:, pl.ds(0, HALO), :] = jnp.zeros((groups, HALO, group), F32)
        ids_ext[pl.ds(0, HALO), :] = jnp.full((HALO, group), -1.0, F32)

    def mail_copy(sent, landed, index, where):
        return remote(
            mail.at[sent], mail.at[landed], mail_send.at[index], mail_recv.at[landed], where
        )

    mail_edge = mail_copy(0, 1, 0, inward)
    mail_in = mail_copy(0, 2, 0, inward)
    mail_out = mail_copy(0, 1, 1, outward)
    mail_relay = [
        mail_copy(1, 3, 2, inward),
        mail_copy(2, 2, 3, outward),
        mail_copy(3, 3, 4, outward),
    ]

    other = (tp + 1) % n_tp
    theirs = pl.multiple_of(other * tokens, tokens)
    mine_at = pl.multiple_of(tp * tokens, tokens)
    act_copy = remote(
        act.at[pl.ds(theirs, tokens)], act_recv, act_sem.at[0], act_sem.at[1], (sp, other)
    )
    lot = tokens // CHUNK
    late = lot + 1

    def conv_step(i, carry):
        @pl.when(i == lot - 1)
        def _():
            pl.semaphore_wait(barrier, per - 1 + 1 + inner_count + has_next + has_last)

            @pl.when(sp < n_sp - 1)
            def _():
                for copy in halo_copies:
                    copy.start()

            @pl.when(edge)
            def _():
                mail_edge.start()

            @pl.when(inner)
            def _():
                mail_in.start()
                mail_out.start()

        @pl.when(i == late)
        def _():
            @pl.when(sp > 0)
            def _():
                for copy in halo_copies:
                    copy.wait_recv()
                for g in range(groups):
                    glu_ext[g, pl.ds(0, HALO), :] = halo_recv[
                        :, g * group : (g + 1) * group
                    ].astype(F32)

        low = (1 - i // lot) * (i + lot) + (i // lot) * (1 - i // late) + (i // (late + 1)) * (
            i - lot
        )
        high = (1 - i // late) * (i + 1) + (i // (late + 1)) * i
        r = pl.multiple_of(((1 - tp) * low + tp * high) * CHUNK, CHUNK)
        mine = ids_here[pl.ds(r, CHUNK), :]
        sums = [jnp.zeros((CHUNK, group), F32) for _ in range(groups)]
        for tap in range(width):
            off = HALO - width + 1 + tap
            same = ids_ext[pl.ds(r + off, CHUNK), :] == mine
            for g in range(groups):
                term = (
                    tap_rows[tap : tap + 1, g * group : (g + 1) * group]
                    * glu_ext[g, pl.ds(r + off, CHUNK), :]
                )
                sums[g] = sums[g] + jnp.where(same, term, 0.0)
        for g in range(groups):
            at = slice(g * group, (g + 1) * group)
            centered = sums[g] - jnp.mean(sums[g], axis=-1, keepdims=True)
            var = jnp.mean(centered * centered, axis=-1, keepdims=True)
            v = centered * lax.rsqrt(var + epsilon) * gain_ref[:, at] + shift_ref[:, at]
            act[pl.ds(r, CHUNK), at] = silu(v).astype(BF16)

        @pl.when((i == lot - 1) & (tp == 0))
        def _():
            act_copy.start()

        @pl.when((i == late) & (tp == 1))
        def _():
            act_copy.start()

        return carry

    lax.fori_loop(0, rows // CHUNK, conv_step, 0)

    @pl.when(inner)
    def _():
        mail_copy(1, 1, 0, inward).wait_recv()
        mail_relay[0].start()
        mail_copy(2, 2, 0, inward).wait_recv()
        mail_relay[1].start()

    loads[10].wait()
    projected = jnp.dot(
        act[pl.ds(mine_at, tokens), :],
        conv_out[pl.ds(pl.multiple_of(tp * channels, channels), channels), :],
        preferred_element_type=F32,
    )
    act_copy.wait_recv()
    projected = projected + jnp.dot(
        act_recv[...],
        conv_out[pl.ds(pl.multiple_of(other * channels, channels), channels), :],
        preferred_element_type=F32,
    )
    stream = (resid_ref[...].astype(F32) + projected).astype(BF16).astype(F32)
    base_ref[...] = stream
    normed = (
        stream
        * lax.rsqrt(jnp.mean(stream * stream, axis=-1, keepdims=True) + epsilon)
        * ngain_ref[...]
    ).astype(BF16)
    for q in range(PARTS):
        tok[0, q] = normed[:, q * cols : (q + 1) * cols]

    first = plane * per
    tri_r = lax.broadcasted_iota(jnp.int32, (tokens, tokens), 0)
    tri_c = lax.broadcasted_iota(jnp.int32, (tokens, tokens), 1)
    later = (tri_r < tri_c).astype(F32).astype(BF16)
    spread_t = (
        (
            lax.broadcasted_iota(jnp.int32, (slots, per), 0) // capacity
            == lax.broadcasted_iota(jnp.int32, (slots, per), 1)
        )
        .astype(F32)
        .astype(BF16)
    )
    row_slot = (lax.broadcasted_iota(jnp.int32, (slots, tokens), 0) % capacity).astype(F32)
    row_expert = (
        first + lax.broadcasted_iota(jnp.int32, (slots, tokens), 0) // capacity
    ).astype(F32)
    expert_row = (first + lax.broadcasted_iota(jnp.int32, (per, tokens), 0)).astype(F32)

    def tables(b):
        routes, weight = mail[b, 0:2, :], mail[b, 2:4, :]
        member = (
            (routes[0:1, :] == expert_row).astype(F32)
            + (routes[1:2, :] == expert_row).astype(F32)
        ).astype(BF16)
        slot = jnp.dot(member, later, preferred_element_type=F32).astype(BF16)
        right = jnp.dot(spread_t, slot, preferred_element_type=F32) == row_slot
        hit0 = jnp.where(right & (routes[0:1, :] == row_expert), 1.0, 0.0)
        hit1 = jnp.where(right & (routes[1:2, :] == row_expert), 1.0, 0.0)
        picks[b] = (hit0 + hit1).astype(BF16)
        mix = (hit0 * weight[0:1, :] + hit1 * weight[1:2, :]).T
        high = mix.astype(BF16)
        highs[b] = high
        lows[b] = (mix - high.astype(F32)).astype(BF16)

    def piece(index):
        return pl.ds(pl.multiple_of(index * capacity, capacity), capacity)

    most = pl.ds(0, (per - 1) * capacity)

    def tok_copy(sent, landed, index, q, where):
        return remote(
            tok.at[sent, q], tok.at[landed, q], tok_send.at[index, q], tok_recv.at[landed, q], where
        )

    def part_copy(b, landed, q, where):
        return remote(
            partial.at[b, q], inc.at[landed, q], part_send.at[b, q], part_recv.at[landed, q], where
        )

    def out_copy(q):
        return pltpu.make_async_copy(
            out_ref.at[q], out_hbm.at[:, pl.ds(q * cols, cols)], out_sem.at[q]
        )

    own_links = {
        "E": ((0, 1, 0, inward),),
        "I": ((0, 2, 0, inward), (0, 1, 1, outward)),
    }
    relays = {
        "E": {},
        "I": {1: (1, 3, 2, inward), 2: (2, 2, 3, outward), 3: (3, 3, 4, outward)},
    }
    part_links = {
        "E": {1: (0, inward), 2: (2, inward), 3: (3, inward)},
        "I": {1: (0, outward), 2: (1, inward), 3: (4, inward)},
    }
    joins = {"E": {1: None, 2: None, 3: None}, "I": {1: 4, 2: 2, 3: 3}}
    closes = {"E": (0,), "I": (0, 1)}

    def arrive(sem, buffer, b, q):
        area = buffer.at[b, q, most]
        remote(area, area, sem.at[b, q], sem.at[b, q], inward).wait_recv()

    def exchange(src, dst, sems, b, q):
        for peer in peers:
            remote(
                src.at[b, q, piece(peer)],
                dst.at[b, q, piece(here)],
                sems[0].at[b, q],
                sems[1].at[b, q],
                peer_place(peer),
            ).start()
        dst[b, q, piece(here), :] = src[b, q, piece(here), :]

    def op(role, kind, b, q):
        if kind == "D":
            for sent, landed, index, where in own_links[role][b : b + 1]:
                tok_copy(sent, landed, index, q, where).start()
        elif kind == "T":
            if role == "E":
                mail_copy(b, b, 0, inward).wait_recv()
            tables(b)
        elif kind == "R":
            mail_copy(3, 3, 0, inward).wait_recv()
            mail_relay[2].start()
        elif kind == "L":
            tok_copy(b, b, 0, q, inward).wait_recv()
            sent, landed, index, where = relays[role][b]
            tok_copy(sent, landed, index, q, where).start()
        elif kind == "P":
            if role == "E" and b:
                tok_copy(b, b, 0, q, inward).wait_recv()
            outgoing[b, q] = jnp.dot(picks[b], tok[b, q], preferred_element_type=F32).astype(BF16)
            exchange(outgoing, arrived, (go_send, go_recv), b, q)
        elif kind == "S":
            gate = jnp.zeros((tokens, sg.shape[1]), F32)
            up = jnp.zeros((tokens, sg.shape[1]), F32)
            for p in range(PARTS):
                k = slice(p * cols, (p + 1) * cols)
                gate = gate + jnp.dot(tok[0, p], sg[k, :], preferred_element_type=F32)
                up = up + jnp.dot(tok[0, p], su[k, :], preferred_element_type=F32)
            hidden = (silu(gate) * up).astype(BF16)
            base_ref[...] += jnp.dot(hidden, sd[...], preferred_element_type=F32)
        elif kind == "X":
            gate = jnp.zeros((slots, eg.shape[2]), F32)
            up = jnp.zeros((slots, eg.shape[2]), F32)
            for p in range(PARTS):
                k = slice(p * cols, (p + 1) * cols)
                arrive(go_recv, arrived, b, p)
                gate = gate + jnp.dot(arrived[b, p], eg[0, k, :], preferred_element_type=F32)
                up = up + jnp.dot(arrived[b, p], eu[0, k, :], preferred_element_type=F32)
            hidden = (silu(gate) * up).astype(BF16)
            for p in range(PARTS):
                k = slice(p * cols, (p + 1) * cols)
                result[b, p] = jnp.dot(
                    hidden, ed[0, :, k], preferred_element_type=F32
                ).astype(BF16)
                exchange(result, returned, (back_send, back_recv), b, p)
        elif kind == "M":
            arrive(back_recv, returned, b, q)
            back = returned[b, q]
            mixed = jnp.dot(highs[b], back, preferred_element_type=F32) + jnp.dot(
                lows[b], back, preferred_element_type=F32
            )
            if b == 0:
                base_ref[:, q * cols : (q + 1) * cols] += mixed
                return
            joined = joins[role][b]
            if joined is not None:
                part_copy(b, joined, q, inward).wait_recv()
                mixed = mixed + inc[joined, q].astype(F32)
            partial[b, q] = mixed.astype(BF16)
            landed, where = part_links[role][b]
            part_copy(b, landed, q, where).start()
        elif kind == "F":
            total = base_ref[:, q * cols : (q + 1) * cols]
            for joined in closes[role]:
                part_copy(1, joined, q, inward).wait_recv()
                total = total + inc[joined, q].astype(F32)
            out_ref[q] = total.astype(BF16)
            out_copy(q).start()

    def close(role):
        for sent, landed, index, where in own_links[role]:
            for q in range(PARTS):
                tok_copy(sent, landed, index, q, where).wait_send()
        for sent, landed, index, where in relays[role].values():
            for q in range(PARTS):
                tok_copy(sent, landed, index, q, where).wait_send()
        for b, (landed, where) in part_links[role].items():
            for q in range(PARTS):
                part_copy(b, landed, q, where).wait_send()

    tables(0)
    for load in loads[11:]:
        load.wait()
    for role, chosen in (("E", edge), ("I", inner)):

        @pl.when(chosen)
        def _(role=role):
            for step in ORDERS[role]:
                op(role, step[0], int(step[1]), int(step[2]))
            close(role)

    @pl.when(edge)
    def _():
        mail_edge.wait_send()

    @pl.when(inner)
    def _():
        mail_in.wait_send()
        mail_out.wait_send()
        for copy in mail_relay:
            copy.wait_send()

    act_copy.wait_send()

    @pl.when(sp < n_sp - 1)
    def _():
        for copy in halo_copies:
            copy.wait_send()

    for b in range(PLANES):
        for q in range(PARTS):
            for sem, buffer in ((go_send, outgoing), (back_send, result)):
                remote(
                    buffer.at[b, q, most], buffer.at[b, q, most], sem.at[b, q], sem.at[b, q], inward
                ).wait_send()
    for q in range(PARTS):
        out_copy(q).wait()


def fused(
    conv_value,
    conv_gate,
    taps,
    doc_ids,
    gn_gain,
    gn_shift,
    conv_out,
    residual,
    norm_gain,
    routes,
    route_weight,
    expert_gate,
    expert_up,
    expert_down,
    shared_gate,
    shared_up,
    shared_down,
):
    n_sp, n_tp = lax.axis_size("sp"), lax.axis_size("tp")
    n = n_sp * n_tp
    rows, channels = conv_value.shape
    tokens, model = residual.shape
    capacity = 2 * tokens * routes.shape[1] // n
    group = channels * n_tp // GROUPS
    slots = n // PLANES * capacity
    cols = model // PARTS
    operands = (
        conv_value,
        conv_gate,
        taps,
        doc_ids[None, :],
        gn_gain[None, :],
        gn_shift[None, :],
        residual,
        norm_gain[None, :],
        routes.T,
        route_weight.T,
        conv_out,
        shared_gate,
        shared_up,
        shared_down,
        expert_gate,
        expert_up,
        expert_down,
    )
    hbm = pl.BlockSpec(memory_space=pl.ANY)
    dma = pltpu.SemaphoreType.DMA
    return pl.pallas_call(
        functools.partial(fused_kernel, n_sp, n_tp, capacity),
        out_shape=jax.ShapeDtypeStruct((tokens, model), BF16),
        in_specs=[hbm] * len(operands),
        out_specs=hbm,
        scratch_shapes=[pltpu.VMEM(x.shape, x.dtype) for x in operands]
        + [
            pltpu.VMEM((channels // group, rows + HALO, group), F32),
            pltpu.VMEM((rows + HALO, group), F32),
            pltpu.VMEM((taps.shape[0] + 1, channels), F32),
            pltpu.VMEM((HALO, channels), BF16),
            pltpu.VMEM((HALO, channels), BF16),
            pltpu.VMEM((rows, channels), BF16),
            pltpu.VMEM((tokens, channels), BF16),
            pltpu.VMEM((rows, group), F32),
            pltpu.VMEM((tokens, model), F32),
            pltpu.VMEM((PLANES, 4, tokens), F32),
            pltpu.VMEM((PLANES, slots, tokens), BF16),
            pltpu.VMEM((PLANES, tokens, slots), BF16),
            pltpu.VMEM((PLANES, tokens, slots), BF16),
            pltpu.VMEM((PLANES, PARTS, tokens, cols), BF16),
            pltpu.VMEM((PLANES, PARTS, slots, cols), BF16),
            pltpu.VMEM((PLANES, PARTS, slots, cols), BF16),
            pltpu.VMEM((PLANES, PARTS, slots, cols), BF16),
            pltpu.VMEM((PLANES, PARTS, slots, cols), BF16),
            pltpu.VMEM((PLANES, PARTS, tokens, cols), BF16),
            pltpu.VMEM((5, PARTS, tokens, cols), BF16),
            pltpu.VMEM((PARTS, tokens, cols), BF16),
            dma((17,)),
            dma((4,)),
            dma((2,)),
            dma((5,)),
            dma((PLANES,)),
            dma((5, PARTS)),
            dma((PLANES, PARTS)),
            dma((PLANES, PARTS)),
            dma((PLANES, PARTS)),
            dma((PLANES, PARTS)),
            dma((PLANES, PARTS)),
            dma((PLANES, PARTS)),
            dma((5, PARTS)),
            dma((PARTS,)),
        ],
        compiler_params=pltpu.CompilerParams(
            collective_id=0, has_side_effects=True, vmem_limit_bytes=VMEM_LIMIT
        ),
    )(*operands)


def fits(mesh):
    n = mesh.size
    return n & (n - 1) == 0 and 8 < n <= 32 and mesh.shape["tp"] == 2


def solution(mesh):
    return jax.shard_map(
        fused if fits(mesh) else per_device,
        mesh=mesh,
        in_specs=(
            P("sp", "tp"),
            P("sp", "tp"),
            P(None, "tp"),
            P("sp"),
            P("tp"),
            P("tp"),
            P(),
            P(("sp", "tp"), None),
            P(),
            P(("sp", "tp"), None),
            P(("sp", "tp"), None),
            P(("sp", "tp"), None, None),
            P(("sp", "tp"), None, None),
            P(("sp", "tp"), None, None),
            P(),
            P(),
            P(),
        ),
        out_specs=P(("sp", "tp"), None),
        check_vma=False,
    )
```

```python
import functools

import jax
import jax.numpy as jnp
from jax import lax
from jax.experimental import pallas as pl
from jax.experimental.pallas import tpu as pltpu
from jax.sharding import PartitionSpec as P

GROUPS = 8


epsilon = 1e-06


def from_behind(x, axis, by):
    peers = lax.axis_size(axis)
    pairs = [(i, i + by) for i in range(peers) if 0 <= i + by < peers]
    return lax.ppermute(x, axis, pairs)


def per_device(
    conv_value,
    conv_gate,
    taps,
    doc_ids,
    gn_gain,
    gn_shift,
    conv_out,
    residual,
    norm_gain,
    routes,
    route_weight,
    expert_gate,
    expert_up,
    expert_down,
    shared_gate,
    shared_up,
    shared_down,
):
    position_count, channel_count = conv_value.shape
    kernel_width = taps.shape[0]
    model_width = residual.shape[1]
    glu_out = (
        conv_value.astype(jnp.float32) * jax.nn.sigmoid(conv_gate.astype(jnp.float32))
    ).astype(jnp.bfloat16)
    rim_start = position_count - kernel_width + 1
    edge_glu, edge_ids = from_behind((glu_out[rim_start:], doc_ids[rim_start:]), "sp", 1)
    longer_glu = jnp.concatenate([edge_glu, glu_out], axis=0)
    longer_ids = jnp.concatenate([edge_ids, doc_ids], axis=0)
    conv_sum = jnp.zeros((position_count, channel_count), jnp.float32)
    for offset in range(kernel_width):
        same_doc = (longer_ids[offset : offset + position_count] == doc_ids)[:, None]
        tap_term = taps[offset].astype(jnp.float32)[None, :] * longer_glu[
            offset : offset + position_count
        ].astype(jnp.float32)
        conv_sum = conv_sum + jnp.where(same_doc, tap_term, 0.0)
    core_split = lax.axis_size("tp")
    groups_here = GROUPS // core_split
    grouped = conv_sum.reshape(position_count, groups_here, channel_count // groups_here)
    group_mean = jnp.mean(grouped, axis=-1, keepdims=True)
    centered = grouped - group_mean
    group_var = jnp.mean(centered * centered, axis=-1, keepdims=True)
    normalized = (centered * lax.rsqrt(group_var + epsilon)).reshape(position_count, channel_count)
    conv_act = jax.nn.silu(normalized * gn_gain + gn_shift).astype(jnp.bfloat16)
    token_rows = lax.all_to_all(conv_act, "tp", split_axis=0, concat_axis=1, tiled=True)
    projected = jnp.dot(token_rows, conv_out, preferred_element_type=jnp.float32)
    stream = (residual.astype(jnp.float32) + projected).astype(jnp.bfloat16)
    stream_wide = stream.astype(jnp.float32)
    normed = (
        stream_wide
        * lax.rsqrt(jnp.mean(stream_wide * stream_wide, axis=-1, keepdims=True) + epsilon)
        * norm_gain
    ).astype(jnp.bfloat16)
    token_count, top_count = routes.shape
    sequence_split = lax.axis_size("sp")
    device_count = sequence_split * core_split
    local_experts = expert_gate.shape[0]
    experts = local_experts * device_count
    capacity = 2 * token_count * top_count // experts
    flat_routes = routes.reshape(-1)
    onehot = (flat_routes[:, None] == jnp.arange(experts, dtype=jnp.int32)[None, :]).astype(
        jnp.int32
    )
    slot_index = jnp.sum(jnp.cumsum(onehot, axis=0) * onehot, axis=1) - 1
    target = flat_routes * capacity + slot_index
    source = (
        jnp.full((experts * capacity,), token_count, jnp.int32)
        .at[target]
        .set(jnp.arange(token_count * top_count, dtype=jnp.int32) // top_count)
    )
    padded_rows = jnp.concatenate([normed, jnp.zeros((1, model_width), normed.dtype)], axis=0)
    outgoing = padded_rows[source]
    shared_hidden = (
        jax.nn.silu(jnp.dot(normed, shared_gate, preferred_element_type=jnp.float32))
        * jnp.dot(normed, shared_up, preferred_element_type=jnp.float32)
    ).astype(jnp.bfloat16)
    shared_out = jnp.dot(shared_hidden, shared_down, preferred_element_type=jnp.float32)
    parcel = outgoing.reshape(device_count, local_experts, capacity, model_width)
    arrived = lax.all_to_all(parcel, ("sp", "tp"), split_axis=0, concat_axis=0, tiled=True)
    expert_rows = arrived[:, 0].reshape(-1, model_width)
    gate_part = jnp.dot(expert_rows, expert_gate[0], preferred_element_type=jnp.float32)
    up_part = jnp.dot(expert_rows, expert_up[0], preferred_element_type=jnp.float32)
    hidden = (jax.nn.silu(gate_part) * up_part).astype(jnp.bfloat16)
    result = jnp.dot(hidden, expert_down[0], preferred_element_type=jnp.float32).astype(
        jnp.bfloat16
    )
    results = [result.reshape(arrived.shape[0], arrived.shape[2], model_width)]
    returned = lax.all_to_all(
        jnp.stack(results, axis=1), ("sp", "tp"), split_axis=0, concat_axis=0, tiled=True
    )
    picked = returned.reshape(experts * capacity, model_width)[target].reshape(
        token_count, top_count, model_width
    )
    routed = jnp.zeros((token_count, model_width), jnp.float32)
    for route_index in range(top_count):
        routed = routed + route_weight[:, route_index, None] * picked[:, route_index].astype(
            jnp.float32
        )
    return (stream_wide + shared_out + routed).astype(jnp.bfloat16)


F32 = jnp.float32
BF16 = jnp.bfloat16
MESH_ID = pl.DeviceIdType.MESH
HALO = 32
CHUNK = 32
PLANES = 4
PARTS = 4
VMEM_LIMIT = 58 * 1024 * 1024


def flip(index, bits):
    out, weight = index, 1
    while weight <= bits:
        if (bits // weight) % 2:
            out = out + weight * (1 - 2 * ((index // weight) % 2))
        weight *= 2
    return out


def silu(v):
    return v / (1.0 + jnp.exp(-v))


ORDERS = {
    "E": (
        (
            "D03", "T20", "D01", "T10", "D02", "P00", "P10", "P02", "D00", "P03", "P12", "P01",
            "P11", "P13", "P22", "X00", "P20", "P23", "X10", "T30", "M03", "P31", "P21", "P33",
            "X01", "M00", "S00", "M10", "P32", "P30", "M12", "X20", "M11", "M13", "M02", "M20",
            "M21", "X30", "M23", "M22", "X31", "M30", "M32", "M33", "M31", "X21", "F00", "X11",
            "F02", "M01", "F01", "F03",
        ),
        (
            "P02", "D01", "P01", "P00", "T20", "P03", "D03", "X01", "X00", "T10", "D02", "T30",
            "X10", "D00", "X20", "P31", "P30", "P33", "P32", "X30", "P23", "X31", "P21", "M03",
            "P22", "M02", "M00", "P20", "S00", "P10", "M01", "M33", "P13", "P11", "M30", "P12",
            "M31", "X21", "M32", "X11", "M20", "M23", "M22", "M21", "M13", "M10", "M12", "F02",
            "M11", "F00", "F01", "F03",
        ),
    ),
    "I": (
        (
            "D02", "D10", "P02", "D12", "D01", "D00", "D11", "T10", "D03", "P00", "L22", "T20",
            "P01", "P22", "R00", "T30", "L13", "D13", "L21", "P13", "P03", "L11", "P11", "L20",
            "P20", "X01", "L12", "L23", "L10", "X00", "L33", "S00", "P12", "P33", "L31", "L32",
            "P23", "P10", "P21", "L30", "P30", "P32", "P31", "X20", "X30", "M20", "X10", "M21",
            "M23", "M22", "M30", "X31", "M32", "M01", "M03", "M33", "X11", "M10", "M31", "F01",
            "M02", "M12", "F02", "F03", "M00", "X21", "M13", "F00", "M11",
        ),
        (
            "P00", "P03", "R00", "P01", "D01", "P02", "X01", "D03", "L21", "T10", "M02", "L11",
            "L12", "L10", "D13", "T30", "L13", "D02", "P13", "M01", "L31", "X10", "T20", "L30",
            "P30", "L33", "L32", "D12", "P33", "L23", "P31", "X20", "D00", "P32", "P21", "P10",
            "X30", "D11", "X00", "P12", "D10", "L22", "S00", "L20", "P11", "P22", "P20", "P23",
            "X31", "X11", "X21", "M30", "M33", "M32", "M31", "M10", "M13", "M12", "M20", "M23",
            "M00", "M03", "M11", "M22", "M21", "F03", "F00", "F02", "F01",
        ),
    ),
}


def fused_kernel(n_sp, n_tp, capacity, *refs):
    hbm_in, out_ref = refs[:17], refs[17]
    vmem_in = refs[18:35]
    (
        glu_ext,
        ids_ext,
        tap_rows,
        halo_send,
        halo_recv,
        act,
        act_recv,
        ids_here,
        base_ref,
        mail,
        picks,
        highs,
        lows,
        tok,
        outgoing,
        arrived,
        result,
        returned,
        partial,
        inc,
        gate_acc,
        up_acc,
        hidden_ref,
        load_sem,
        halo_sem,
        act_sem,
        mail_send,
        mail_recv,
        tok_send,
        tok_recv,
        go_send,
        go_recv,
        back_send,
        back_recv,
        part_send,
        part_recv,
    ) = refs[35:]
    (
        value_ref,
        gate_ref,
        taps_ref,
        ids_ref,
        gain_ref,
        shift_ref,
        resid_ref,
        ngain_ref,
        routes_ref,
        weight_ref,
        conv_out,
        sg,
        su,
        sd,
        eg,
        eu,
        ed,
    ) = vmem_in
    n = n_sp * n_tp
    per = n // PLANES
    sp, tp = lax.axis_index("sp"), lax.axis_index("tp")
    me = sp * n_tp + tp
    plane, here = me // per, me % per
    rows, channels = value_ref.shape
    tokens, model = resid_ref.shape
    width = taps_ref.shape[0]
    group = glu_ext.shape[2]
    groups = channels // group
    cols = model // PARTS
    slots = per * capacity
    side = 1 - 2 * (plane // 2)
    edge = plane % (PLANES - 1) == 0
    inner = plane % (PLANES - 1) != 0
    inner_count = (plane % (PLANES - 1) + 1) // 2

    def place(index):
        return (index // n_tp, index % n_tp)

    inward = place((plane + side) * per + here)
    outward = place((plane - side) * per + here)
    peers = [flip(here, k) for k in range(per - 1, 0, -1)]

    def peer_place(peer):
        return place(plane * per + peer)

    loads = [
        pltpu.make_async_copy(a, b, load_sem.at[i])
        for i, (a, b) in enumerate(zip(hbm_in, vmem_in))
    ]
    barrier = pltpu.get_barrier_semaphore()

    def greet(where):
        pl.semaphore_signal(barrier, inc=1, device_id=where, device_id_type=MESH_ID)

    for load in loads:
        load.start()
    for peer in peers:
        greet(peer_place(peer))
    greet(inward)

    @pl.when(inner)
    def _():
        greet(outward)

    @pl.when(sp < n_sp - 1)
    def _():
        greet((sp + 1, tp))

    @pl.when(sp > 0)
    def _():
        greet((sp - 1, tp))

    has_next = 1 - (sp + 1) // n_sp
    has_last = (sp + n_sp - 1) // n_sp
    for load in loads[:10]:
        load.wait()

    mail[0, 0:2, :] = routes_ref[...].astype(F32)
    mail[0, 2:4, :] = weight_ref[...]
    glu = (value_ref[...].astype(F32) * jax.nn.sigmoid(gate_ref[...].astype(F32))).astype(BF16)
    halo_send[...] = glu[rows - HALO :, :]
    for g in range(groups):
        glu_ext[g, pl.ds(HALO, rows), :] = glu[:, g * group : (g + 1) * group].astype(F32)
    for at in range(0, rows, group):
        row = ids_ref[:, at : at + group].astype(F32)
        column = jnp.broadcast_to(row, (group, group)).T
        ids_here[pl.ds(at, group), :] = column
        ids_ext[pl.ds(HALO + at, group), :] = column
    tap_rows[pl.ds(0, width), :] = taps_ref[...].astype(F32)

    def remote(src, dst, send_sem, recv_sem, where):
        return pltpu.make_async_remote_copy(
            src_ref=src,
            dst_ref=dst,
            send_sem=send_sem,
            recv_sem=recv_sem,
            device_id=where,
            device_id_type=MESH_ID,
        )

    halo_copies = [
        remote(halo_send, halo_recv, halo_sem.at[0], halo_sem.at[1], (sp + 1, tp)),
        remote(
            ids_here.at[pl.ds(rows - HALO, HALO)],
            ids_ext.at[pl.ds(0, HALO)],
            halo_sem.at[2],
            halo_sem.at[3],
            (sp + 1, tp),
        ),
    ]

    @pl.when(sp == 0)
    def _():
        glu_ext[:, pl.ds(0, HALO), :] = jnp.zeros((groups, HALO, group), F32)
        ids_ext[pl.ds(0, HALO), :] = jnp.full((HALO, group), -1.0, F32)

    def mail_copy(sent, landed, index, where):
        return remote(
            mail.at[sent], mail.at[landed], mail_send.at[index], mail_recv.at[landed], where
        )

    mail_edge = mail_copy(0, 1, 0, inward)
    mail_in = mail_copy(0, 2, 0, inward)
    mail_out = mail_copy(0, 1, 1, outward)
    mail_relay = [
        mail_copy(1, 3, 2, inward),
        mail_copy(2, 2, 3, outward),
        mail_copy(3, 3, 4, outward),
    ]

    other = (tp + 1) % n_tp
    theirs = pl.multiple_of(other * tokens, tokens)
    mine_at = pl.multiple_of(tp * tokens, tokens)
    act_copy = remote(
        act.at[pl.ds(theirs, tokens)], act_recv, act_sem.at[0], act_sem.at[1], (sp, other)
    )
    lot = tokens // CHUNK
    late = lot + 2

    def conv_step(i, carry):
        @pl.when(i == 0)
        def _():
            pl.semaphore_wait(barrier, per - 1 + 1 + inner_count + has_next + has_last)

            @pl.when(sp < n_sp - 1)
            def _():
                for copy in halo_copies:
                    copy.start()

            @pl.when(edge)
            def _():
                mail_edge.start()

            @pl.when(inner)
            def _():
                mail_in.start()
                mail_out.start()

        @pl.when(i == late)
        def _():
            @pl.when(sp > 0)
            def _():
                for copy in halo_copies:
                    copy.wait_recv()
                for g in range(groups):
                    glu_ext[g, pl.ds(0, HALO), :] = halo_recv[
                        :, g * group : (g + 1) * group
                    ].astype(F32)

        low = (
            (1 - i // lot) * (i + lot)
            + (i // lot) * (1 - i // late) * (i - lot + 1)
            + (i // (late + 1)) * (i - lot)
        )
        high = (1 - i // late) * (i + 1) + (i // (late + 1)) * i
        r = pl.multiple_of(((1 - tp) * low + tp * high) * CHUNK, CHUNK)
        mine = ids_here[pl.ds(r, CHUNK), :]
        sums = [jnp.zeros((CHUNK, group), F32) for _ in range(groups)]
        for tap in range(width):
            off = HALO - width + 1 + tap
            same = ids_ext[pl.ds(r + off, CHUNK), :] == mine
            for g in range(groups):
                term = (
                    tap_rows[tap : tap + 1, g * group : (g + 1) * group]
                    * glu_ext[g, pl.ds(r + off, CHUNK), :]
                )
                sums[g] = sums[g] + jnp.where(same, term, 0.0)
        for g in range(groups):
            at = slice(g * group, (g + 1) * group)
            centered = sums[g] - jnp.mean(sums[g], axis=-1, keepdims=True)
            var = jnp.mean(centered * centered, axis=-1, keepdims=True)
            v = centered * lax.rsqrt(var + epsilon) * gain_ref[:, at] + shift_ref[:, at]
            act[pl.ds(r, CHUNK), at] = silu(v).astype(BF16)

        @pl.when((i == lot - 1) & (tp == 0))
        def _():
            act_copy.start()

        @pl.when((i == late) & (tp == 1))
        def _():
            act_copy.start()

        return carry

    lax.fori_loop(0, rows // CHUNK, conv_step, 0)

    @pl.when(inner)
    def _():
        mail_copy(1, 1, 0, inward).wait_recv()
        mail_relay[0].start()
        mail_copy(2, 2, 0, inward).wait_recv()
        mail_relay[1].start()

    loads[10].wait()
    projected = jnp.dot(
        act[pl.ds(mine_at, tokens), :],
        conv_out[pl.ds(pl.multiple_of(tp * channels, channels), channels), :],
        preferred_element_type=F32,
    )
    act_copy.wait_recv()
    projected = projected + jnp.dot(
        act_recv[...],
        conv_out[pl.ds(pl.multiple_of(other * channels, channels), channels), :],
        preferred_element_type=F32,
    )
    stream = (resid_ref[...].astype(F32) + projected).astype(BF16).astype(F32)
    normed = (
        stream
        * lax.rsqrt(jnp.mean(stream * stream, axis=-1, keepdims=True) + epsilon)
        * ngain_ref[...]
    ).astype(BF16)
    for q in range(PARTS):
        tok[0, q] = normed[:, q * cols : (q + 1) * cols]
        base_ref[q] = stream[:, q * cols : (q + 1) * cols]

    first = plane * per
    tri_r = lax.broadcasted_iota(jnp.int32, (tokens, tokens), 0)
    tri_c = lax.broadcasted_iota(jnp.int32, (tokens, tokens), 1)
    later = (tri_r < tri_c).astype(F32).astype(BF16)
    spread_t = (
        (
            lax.broadcasted_iota(jnp.int32, (slots, per), 0) // capacity
            == lax.broadcasted_iota(jnp.int32, (slots, per), 1)
        )
        .astype(F32)
        .astype(BF16)
    )
    row_slot = (lax.broadcasted_iota(jnp.int32, (slots, tokens), 0) % capacity).astype(F32)
    row_expert = (
        first + lax.broadcasted_iota(jnp.int32, (slots, tokens), 0) // capacity
    ).astype(F32)
    expert_row = (first + lax.broadcasted_iota(jnp.int32, (per, tokens), 0)).astype(F32)

    def tables(b):
        routes, weight = mail[b, 0:2, :], mail[b, 2:4, :]
        member = (
            (routes[0:1, :] == expert_row).astype(F32)
            + (routes[1:2, :] == expert_row).astype(F32)
        ).astype(BF16)
        slot = jnp.dot(member, later, preferred_element_type=F32).astype(BF16)
        right = jnp.dot(spread_t, slot, preferred_element_type=F32) == row_slot
        hit0 = jnp.where(right & (routes[0:1, :] == row_expert), 1.0, 0.0)
        hit1 = jnp.where(right & (routes[1:2, :] == row_expert), 1.0, 0.0)
        picks[b] = (hit0 + hit1).astype(BF16)
        mix = (hit0 * weight[0:1, :] + hit1 * weight[1:2, :]).T
        high = mix.astype(BF16)
        highs[b] = high
        lows[b] = (mix - high.astype(F32)).astype(BF16)

    def piece(index):
        return pl.ds(pl.multiple_of(index * capacity, capacity), capacity)

    chips = per // n_tp
    lane = chips * capacity
    chip = here // n_tp
    mine_row = tp * chips + chip

    def toward(sign):
        return place((plane + side * sign) * per + here)

    def tok_copy(sent, landed, index, q, where):
        return remote(
            tok.at[sent, q], tok.at[landed, q], tok_send.at[index, q], tok_recv.at[landed, q], where
        )

    def part_copy(b, landed, q, where):
        return remote(
            partial.at[b, q], inc.at[landed, q], part_send.at[b, q], part_recv.at[landed, q], where
        )

    def bytes_of(buffer, b, q, count, sem):
        area = buffer.at[b, q, pl.ds(0, count * capacity)]
        return remote(area, area, sem, sem, inward)

    def send_rows(core, b, q):
        for peer in peers:
            remote(
                outgoing.at[b, q, piece(peer)],
                arrived.at[b, q, piece(mine_row)],
                go_send.at[b, q],
                go_recv.at[b, q, core],
                peer_place(peer),
            ).start()
        arrived[b, q, piece(mine_row), :] = outgoing[b, q, piece(here), :]

    def return_rows(core, b, q, s):
        for apart in range(chips - 1, -1, -1):
            target = flip(chip, apart)
            if apart == 0 and s == core:
                returned[b, q, piece(here), :] = result[b, q, piece(mine_row), :]
            else:
                remote(
                    result.at[b, q, piece(s * chips + target)],
                    returned.at[b, q, piece(here)],
                    back_send.at[b, q],
                    back_recv.at[b, q],
                    peer_place(target * n_tp + s),
                ).start()

    landing = {"E": {0: (1, 1)}, "I": {0: (2, 1), 1: (1, -1)}}
    relaying = {1: (3, 2, 1), 2: (2, 3, -1), 3: (3, 4, -1)}
    part_to = {
        "E": {1: (0, 1), 2: (2, 1), 3: (3, 1)},
        "I": {1: (0, -1), 2: (1, 1), 3: (4, 1)},
    }
    joins = {1: 4, 2: 2, 3: 3}
    closes = {"E": (0,), "I": (0, 1)}

    def op(role, core, kind, b, q):
        if kind == "D":
            landed, sign = landing[role][b]
            tok_copy(0, landed, b, q, toward(sign)).start()
        elif kind == "T":
            if role == "E":
                mail_copy(b, b, 0, inward).wait_recv()
            tables(b)
        elif kind == "R":
            mail_copy(3, 3, 0, inward).wait_recv()
            mail_relay[2].start()
        elif kind == "L":
            tok_copy(b, b, 0, q, inward).wait_recv()
            landed, index, sign = relaying[b]
            tok_copy(b, landed, index, q, toward(sign)).start()
        elif kind == "P":
            if role == "E" and b:
                tok_copy(b, b, 0, q, inward).wait_recv()
            outgoing[b, q] = jnp.dot(picks[b], tok[b, q], preferred_element_type=F32).astype(BF16)
            send_rows(core, b, q)
        elif kind == "S":
            gate = jnp.zeros((tokens, sg.shape[1]), F32)
            up = jnp.zeros((tokens, sg.shape[1]), F32)
            for p in range(PARTS):
                k = slice(p * cols, (p + 1) * cols)
                gate = gate + jnp.dot(tok[0, p], sg[k, :], preferred_element_type=F32)
                up = up + jnp.dot(tok[0, p], su[k, :], preferred_element_type=F32)
            hidden = (silu(gate) * up).astype(BF16)
            for p in range(PARTS):
                k = slice(p * cols, (p + 1) * cols)
                base_ref[p] += jnp.dot(hidden, sd[:, k], preferred_element_type=F32)
        elif kind == "X":
            s, at = q, slice(q * lane, (q + 1) * lane)
            count = chips - int(s == core)
            gate_acc[...] = jnp.zeros((lane, eg.shape[2]), F32)
            up_acc[...] = jnp.zeros((lane, eg.shape[2]), F32)

            def widen(p, carry):
                k = pl.ds(pl.multiple_of(p * cols, cols), cols)
                bytes_of(arrived, b, p, count, go_recv.at[b, p, s]).wait_recv()
                x = arrived[b, p, at, :]
                gate_acc[...] += jnp.dot(x, eg[0, k, :], preferred_element_type=F32)
                up_acc[...] += jnp.dot(x, eu[0, k, :], preferred_element_type=F32)
                return carry

            lax.fori_loop(0, PARTS, widen, 0, unroll=2)
            hidden_ref[...] = (silu(gate_acc[...]) * up_acc[...]).astype(BF16)

            def narrow(p, carry):
                k = pl.ds(pl.multiple_of(p * cols, cols), cols)
                result[b, p, at, :] = jnp.dot(
                    hidden_ref[...], ed[0, :, k], preferred_element_type=F32
                ).astype(BF16)
                return_rows(core, b, p, s)
                return carry

            lax.fori_loop(0, PARTS, narrow, 0, unroll=2)
        elif kind == "M":
            bytes_of(returned, b, q, per - 1, back_recv.at[b, q]).wait_recv()
            back = returned[b, q]
            mixed = jnp.dot(highs[b], back, preferred_element_type=F32) + jnp.dot(
                lows[b], back, preferred_element_type=F32
            )
            if b == 0:
                base_ref[q] += mixed
                return
            if role == "I":
                joined = joins[b]
                part_copy(b, joined, q, inward).wait_recv()
                mixed = mixed + inc[joined, q].astype(F32)
            partial[b, q] = mixed.astype(BF16)
            landed, sign = part_to[role][b]
            part_copy(b, landed, q, toward(sign)).start()
        elif kind == "F":
            total = base_ref[q]
            for joined in closes[role]:
                part_copy(1, joined, q, inward).wait_recv()
                total = total + inc[joined, q].astype(F32)
            out_ref[:, q * cols : (q + 1) * cols] = total.astype(BF16)

    def close(role):
        for index, (landed, sign) in landing[role].items():
            for q in range(PARTS):
                tok_copy(0, landed, index, q, toward(sign)).wait_send()
        for b, (landed, index, sign) in relaying.items():
            if role == "I":
                for q in range(PARTS):
                    tok_copy(b, landed, index, q, toward(sign)).wait_send()
        for b, (landed, sign) in part_to[role].items():
            for q in range(PARTS):
                part_copy(b, landed, q, toward(sign)).wait_send()

    tables(0)
    for load in loads[11:]:
        load.wait()
    for role, chosen in (("E", edge), ("I", inner)):
        for core in range(n_tp):

            @pl.when(chosen & (tp == core))
            def _(role=role, core=core):
                for step in ORDERS[role][core]:
                    op(role, core, step[0], int(step[1]), int(step[2]))
                close(role)

    @pl.when(edge)
    def _():
        mail_edge.wait_send()

    @pl.when(inner)
    def _():
        mail_in.wait_send()
        mail_out.wait_send()
        for copy in mail_relay:
            copy.wait_send()

    act_copy.wait_send()

    @pl.when(sp < n_sp - 1)
    def _():
        for copy in halo_copies:
            copy.wait_send()

    for b in range(PLANES):
        for q in range(PARTS):
            bytes_of(outgoing, b, q, per - 1, go_send.at[b, q]).wait_send()
            bytes_of(result, b, q, per - 1, back_send.at[b, q]).wait_send()


def fused(
    conv_value,
    conv_gate,
    taps,
    doc_ids,
    gn_gain,
    gn_shift,
    conv_out,
    residual,
    norm_gain,
    routes,
    route_weight,
    expert_gate,
    expert_up,
    expert_down,
    shared_gate,
    shared_up,
    shared_down,
):
    n_sp, n_tp = lax.axis_size("sp"), lax.axis_size("tp")
    n = n_sp * n_tp
    rows, channels = conv_value.shape
    tokens, model = residual.shape
    capacity = 2 * tokens * routes.shape[1] // n
    group = channels * n_tp // GROUPS
    slots = n // PLANES * capacity
    cols = model // PARTS
    operands = (
        conv_value,
        conv_gate,
        taps,
        doc_ids[None, :],
        gn_gain[None, :],
        gn_shift[None, :],
        residual,
        norm_gain[None, :],
        routes.T,
        route_weight.T,
        conv_out,
        shared_gate,
        shared_up,
        shared_down,
        expert_gate,
        expert_up,
        expert_down,
    )
    hbm = pl.BlockSpec(memory_space=pl.ANY)
    dma = pltpu.SemaphoreType.DMA
    return pl.pallas_call(
        functools.partial(fused_kernel, n_sp, n_tp, capacity),
        out_shape=pltpu.VMEM((tokens, model), BF16),
        in_specs=[hbm] * len(operands),
        out_specs=pl.BlockSpec(memory_space=pltpu.VMEM),
        scratch_shapes=[pltpu.VMEM(x.shape, x.dtype) for x in operands]
        + [
            pltpu.VMEM((channels // group, rows + HALO, group), F32),
            pltpu.VMEM((rows + HALO, group), F32),
            pltpu.VMEM((taps.shape[0] + 1, channels), F32),
            pltpu.VMEM((HALO, channels), BF16),
            pltpu.VMEM((HALO, channels), BF16),
            pltpu.VMEM((rows, channels), BF16),
            pltpu.VMEM((tokens, channels), BF16),
            pltpu.VMEM((rows, group), F32),
            pltpu.VMEM((PARTS, tokens, cols), F32),
            pltpu.VMEM((PLANES, 4, tokens), F32),
            pltpu.VMEM((PLANES, slots, tokens), BF16),
            pltpu.VMEM((PLANES, tokens, slots), BF16),
            pltpu.VMEM((PLANES, tokens, slots), BF16),
            pltpu.VMEM((PLANES, PARTS, tokens, cols), BF16),
            pltpu.VMEM((PLANES, PARTS, slots, cols), BF16),
            pltpu.VMEM((PLANES, PARTS, slots, cols), BF16),
            pltpu.VMEM((PLANES, PARTS, slots, cols), BF16),
            pltpu.VMEM((PLANES, PARTS, slots, cols), BF16),
            pltpu.VMEM((PLANES, PARTS, tokens, cols), BF16),
            pltpu.VMEM((5, PARTS, tokens, cols), BF16),
            pltpu.VMEM((slots // n_tp, expert_gate.shape[2]), F32),
            pltpu.VMEM((slots // n_tp, expert_gate.shape[2]), F32),
            pltpu.VMEM((slots // n_tp, expert_gate.shape[2]), BF16),
            dma((17,)),
            dma((4,)),
            dma((2,)),
            dma((5,)),
            dma((PLANES,)),
            dma((5, PARTS)),
            dma((PLANES, PARTS)),
            dma((PLANES, PARTS)),
            dma((PLANES, PARTS, n_tp)),
            dma((PLANES, PARTS)),
            dma((PLANES, PARTS)),
            dma((PLANES, PARTS)),
            dma((5, PARTS)),
        ],
        compiler_params=pltpu.CompilerParams(
            collective_id=0, has_side_effects=True, vmem_limit_bytes=VMEM_LIMIT
        ),
    )(*operands)


def fits(mesh):
    n = mesh.size
    return n & (n - 1) == 0 and 8 < n <= 32 and mesh.shape["tp"] == 2


def solution(mesh):
    return jax.shard_map(
        fused if fits(mesh) else per_device,
        mesh=mesh,
        in_specs=(
            P("sp", "tp"),
            P("sp", "tp"),
            P(None, "tp"),
            P("sp"),
            P("tp"),
            P("tp"),
            P(),
            P(("sp", "tp"), None),
            P(),
            P(("sp", "tp"), None),
            P(("sp", "tp"), None),
            P(("sp", "tp"), None, None),
            P(("sp", "tp"), None, None),
            P(("sp", "tp"), None, None),
            P(),
            P(),
            P(),
        ),
        out_specs=P(("sp", "tp"), None),
        check_vma=False,
    )
```

```python
import functools

import jax
import jax.numpy as jnp
from jax import lax
from jax.experimental import pallas as pl
from jax.experimental.pallas import tpu as pltpu
from jax.sharding import PartitionSpec as P

GROUPS = 8


epsilon = 1e-06


def from_behind(x, axis, by):
    peers = lax.axis_size(axis)
    pairs = [(i, i + by) for i in range(peers) if 0 <= i + by < peers]
    return lax.ppermute(x, axis, pairs)


def per_device(
    conv_value,
    conv_gate,
    taps,
    doc_ids,
    gn_gain,
    gn_shift,
    conv_out,
    residual,
    norm_gain,
    routes,
    route_weight,
    expert_gate,
    expert_up,
    expert_down,
    shared_gate,
    shared_up,
    shared_down,
):
    position_count, channel_count = conv_value.shape
    kernel_width = taps.shape[0]
    model_width = residual.shape[1]
    glu_out = (
        conv_value.astype(jnp.float32) * jax.nn.sigmoid(conv_gate.astype(jnp.float32))
    ).astype(jnp.bfloat16)
    rim_start = position_count - kernel_width + 1
    edge_glu, edge_ids = from_behind((glu_out[rim_start:], doc_ids[rim_start:]), "sp", 1)
    longer_glu = jnp.concatenate([edge_glu, glu_out], axis=0)
    longer_ids = jnp.concatenate([edge_ids, doc_ids], axis=0)
    conv_sum = jnp.zeros((position_count, channel_count), jnp.float32)
    for offset in range(kernel_width):
        same_doc = (longer_ids[offset : offset + position_count] == doc_ids)[:, None]
        tap_term = taps[offset].astype(jnp.float32)[None, :] * longer_glu[
            offset : offset + position_count
        ].astype(jnp.float32)
        conv_sum = conv_sum + jnp.where(same_doc, tap_term, 0.0)
    core_split = lax.axis_size("tp")
    groups_here = GROUPS // core_split
    grouped = conv_sum.reshape(position_count, groups_here, channel_count // groups_here)
    group_mean = jnp.mean(grouped, axis=-1, keepdims=True)
    centered = grouped - group_mean
    group_var = jnp.mean(centered * centered, axis=-1, keepdims=True)
    normalized = (centered * lax.rsqrt(group_var + epsilon)).reshape(position_count, channel_count)
    conv_act = jax.nn.silu(normalized * gn_gain + gn_shift).astype(jnp.bfloat16)
    token_rows = lax.all_to_all(conv_act, "tp", split_axis=0, concat_axis=1, tiled=True)
    projected = jnp.dot(token_rows, conv_out, preferred_element_type=jnp.float32)
    stream = (residual.astype(jnp.float32) + projected).astype(jnp.bfloat16)
    stream_wide = stream.astype(jnp.float32)
    normed = (
        stream_wide
        * lax.rsqrt(jnp.mean(stream_wide * stream_wide, axis=-1, keepdims=True) + epsilon)
        * norm_gain
    ).astype(jnp.bfloat16)
    token_count, top_count = routes.shape
    sequence_split = lax.axis_size("sp")
    device_count = sequence_split * core_split
    local_experts = expert_gate.shape[0]
    experts = local_experts * device_count
    capacity = 2 * token_count * top_count // experts
    flat_routes = routes.reshape(-1)
    onehot = (flat_routes[:, None] == jnp.arange(experts, dtype=jnp.int32)[None, :]).astype(
        jnp.int32
    )
    slot_index = jnp.sum(jnp.cumsum(onehot, axis=0) * onehot, axis=1) - 1
    target = flat_routes * capacity + slot_index
    source = (
        jnp.full((experts * capacity,), token_count, jnp.int32)
        .at[target]
        .set(jnp.arange(token_count * top_count, dtype=jnp.int32) // top_count)
    )
    padded_rows = jnp.concatenate([normed, jnp.zeros((1, model_width), normed.dtype)], axis=0)
    outgoing = padded_rows[source]
    shared_hidden = (
        jax.nn.silu(jnp.dot(normed, shared_gate, preferred_element_type=jnp.float32))
        * jnp.dot(normed, shared_up, preferred_element_type=jnp.float32)
    ).astype(jnp.bfloat16)
    shared_out = jnp.dot(shared_hidden, shared_down, preferred_element_type=jnp.float32)
    parcel = outgoing.reshape(device_count, local_experts, capacity, model_width)
    arrived = lax.all_to_all(parcel, ("sp", "tp"), split_axis=0, concat_axis=0, tiled=True)
    expert_rows = arrived[:, 0].reshape(-1, model_width)
    gate_part = jnp.dot(expert_rows, expert_gate[0], preferred_element_type=jnp.float32)
    up_part = jnp.dot(expert_rows, expert_up[0], preferred_element_type=jnp.float32)
    hidden = (jax.nn.silu(gate_part) * up_part).astype(jnp.bfloat16)
    result = jnp.dot(hidden, expert_down[0], preferred_element_type=jnp.float32).astype(
        jnp.bfloat16
    )
    results = [result.reshape(arrived.shape[0], arrived.shape[2], model_width)]
    returned = lax.all_to_all(
        jnp.stack(results, axis=1), ("sp", "tp"), split_axis=0, concat_axis=0, tiled=True
    )
    picked = returned.reshape(experts * capacity, model_width)[target].reshape(
        token_count, top_count, model_width
    )
    routed = jnp.zeros((token_count, model_width), jnp.float32)
    for route_index in range(top_count):
        routed = routed + route_weight[:, route_index, None] * picked[:, route_index].astype(
            jnp.float32
        )
    return (stream_wide + shared_out + routed).astype(jnp.bfloat16)


F32 = jnp.float32
BF16 = jnp.bfloat16
MESH_ID = pl.DeviceIdType.MESH
HALO = 32
CHUNK = 32
PLANES = 4
PARTS = 4
VMEM_LIMIT = 58 * 1024 * 1024


def flip(index, bits):
    out, weight = index, 1
    while weight <= bits:
        if (bits // weight) % 2:
            out = out + weight * (1 - 2 * ((index // weight) % 2))
        weight *= 2
    return out


def silu(v):
    return v / (1.0 + jnp.exp(-v))


ORDERS = {
    "E": (
        (
            "P02", "P03", "P00", "T20", "D00", "P01", "T10", "D02", "D03", "P11", "D01", "P13",
            "P12", "T30", "P10", "X00", "P20", "P21", "P23", "P22", "X10", "P30", "P32", "P33",
            "P31", "M00", "M10", "X20", "M11", "M12", "X30", "M20", "M01", "M22", "M02", "M21",
            "S00", "M23", "X01", "M30", "M33", "M32", "M03", "M31", "X31", "M13", "X21", "F03",
            "X11", "F01", "F00", "F02",
        ),
        (
            "D02", "T20", "S00", "T10", "P00", "P03", "P02", "X00", "D01", "T30", "P01", "D00",
            "X10", "D03", "X20", "P30", "P31", "X30", "P33", "P32", "X01", "P22", "P20", "X31",
            "P23", "P21", "M30", "P12", "M02", "P10", "P11", "M32", "M33", "P13", "X21", "M31",
            "M20", "M00", "M21", "X11", "M22", "M03", "M23", "M10", "M01", "M13", "M12", "F00",
            "F02", "F03", "M11", "F01",
        ),
    ),
    "I": (
        (
            "D01", "D11", "D13", "D12", "S00", "P03", "D00", "P01", "R00", "D02", "T30", "P02",
            "T10", "D10", "T20", "L21", "P00", "D03", "L10", "P21", "L12", "L20", "P12", "P10",
            "P20", "L23", "L13", "L22", "P22", "L32", "L11", "L30", "P13", "X01", "P32", "P11",
            "L33", "P23", "P30", "P33", "L31", "P31", "X00", "X20", "X10", "X30", "M20", "M22",
            "M21", "M23", "M01", "M30", "M02", "M33", "X31", "M32", "M03", "M00", "M10", "M31",
            "F02", "M13", "X11", "M12", "F00", "M11", "X21", "F03", "F01",
        ),
        (
            "P02", "R00", "T10", "P03", "P00", "P01", "T20", "X00", "T30", "L12", "L10", "S00",
            "L11", "D02", "P12", "L13", "D00", "D03", "L30", "P10", "P11", "L31", "P13", "X20",
            "D01", "L32", "L33", "P31", "P32", "L20", "P30", "L22", "P33", "L21", "X30", "D10",
            "P20", "X10", "L23", "P22", "D12", "P23", "D11", "D13", "P21", "X01", "X31", "X11",
            "X21", "M30", "M32", "M33", "M03", "M10", "M31", "M00", "M12", "M13", "M20", "M21",
            "M11", "M02", "M22", "M23", "F00", "F02", "F03", "M01", "F01",
        ),
    ),
}


def fused_kernel(n_sp, n_tp, capacity, *refs):
    hbm_in, out_ref = refs[:17], refs[17]
    vmem_in = refs[18:35]
    (
        glu_ext,
        ids_ext,
        tap_rows,
        halo_send,
        halo_recv,
        act,
        act_recv,
        ids_here,
        base_ref,
        mail,
        picks,
        highs,
        lows,
        tok,
        outgoing,
        arrived,
        result,
        returned,
        partial,
        inc,
        gate_acc,
        up_acc,
        hidden_ref,
        load_sem,
        halo_sem,
        act_sem,
        mail_send,
        mail_recv,
        tok_send,
        tok_recv,
        go_send,
        go_recv,
        back_send,
        back_recv,
        part_send,
        part_recv,
    ) = refs[35:]
    (
        value_ref,
        gate_ref,
        taps_ref,
        ids_ref,
        gain_ref,
        shift_ref,
        resid_ref,
        ngain_ref,
        routes_ref,
        weight_ref,
        conv_out,
        sg,
        su,
        sd,
        eg,
        eu,
        ed,
    ) = vmem_in
    n = n_sp * n_tp
    per = n // PLANES
    sp, tp = lax.axis_index("sp"), lax.axis_index("tp")
    me = sp * n_tp + tp
    plane, here = me // per, me % per
    rows, channels = value_ref.shape
    tokens, model = resid_ref.shape
    width = taps_ref.shape[0]
    group = glu_ext.shape[2]
    groups = channels // group
    cols = model // PARTS
    slots = per * capacity
    side = 1 - 2 * (plane // 2)
    edge = plane % (PLANES - 1) == 0
    inner = plane % (PLANES - 1) != 0
    inner_count = (plane % (PLANES - 1) + 1) // 2

    def place(index):
        return (index // n_tp, index % n_tp)

    inward = place((plane + side) * per + here)
    outward = place((plane - side) * per + here)
    peers = [flip(here, k) for k in range(per - 1, 0, -1)]

    def peer_place(peer):
        return place(plane * per + peer)

    loads = [
        pltpu.make_async_copy(a, b, load_sem.at[i])
        for i, (a, b) in enumerate(zip(hbm_in, vmem_in))
    ]
    barrier = pltpu.get_barrier_semaphore()

    def greet(where):
        pl.semaphore_signal(barrier, inc=1, device_id=where, device_id_type=MESH_ID)

    for load in loads:
        load.start()
    for peer in peers:
        greet(peer_place(peer))
    greet(inward)

    @pl.when(inner)
    def _():
        greet(outward)

    @pl.when(sp < n_sp - 1)
    def _():
        greet((sp + 1, tp))

    @pl.when(sp > 0)
    def _():
        greet((sp - 1, tp))

    has_next = 1 - (sp + 1) // n_sp
    has_last = (sp + n_sp - 1) // n_sp
    for load in loads[:10]:
        load.wait()

    mail[0, 0:2, :] = routes_ref[...].astype(F32)
    mail[0, 2:4, :] = weight_ref[...]
    glu = (value_ref[...].astype(F32) * jax.nn.sigmoid(gate_ref[...].astype(F32))).astype(BF16)
    halo_send[...] = glu[rows - HALO :, :]
    for g in range(groups):
        glu_ext[g, pl.ds(HALO, rows), :] = glu[:, g * group : (g + 1) * group].astype(F32)
    for at in range(0, rows, group):
        row = ids_ref[:, at : at + group].astype(F32)
        column = jnp.broadcast_to(row, (group, group)).T
        ids_here[pl.ds(at, group), :] = column
        ids_ext[pl.ds(HALO + at, group), :] = column
    tap_rows[pl.ds(0, width), :] = taps_ref[...].astype(F32)

    def remote(src, dst, send_sem, recv_sem, where):
        return pltpu.make_async_remote_copy(
            src_ref=src,
            dst_ref=dst,
            send_sem=send_sem,
            recv_sem=recv_sem,
            device_id=where,
            device_id_type=MESH_ID,
        )

    halo_copies = [
        remote(halo_send, halo_recv, halo_sem.at[0], halo_sem.at[1], (sp + 1, tp)),
        remote(
            ids_here.at[pl.ds(rows - HALO, HALO)],
            ids_ext.at[pl.ds(0, HALO)],
            halo_sem.at[2],
            halo_sem.at[3],
            (sp + 1, tp),
        ),
    ]

    @pl.when(sp == 0)
    def _():
        glu_ext[:, pl.ds(0, HALO), :] = jnp.zeros((groups, HALO, group), F32)
        ids_ext[pl.ds(0, HALO), :] = jnp.full((HALO, group), -1.0, F32)

    def mail_copy(sent, landed, index, where):
        return remote(
            mail.at[sent], mail.at[landed], mail_send.at[index], mail_recv.at[landed], where
        )

    mail_edge = mail_copy(0, 1, 0, inward)
    mail_in = mail_copy(0, 2, 0, inward)
    mail_out = mail_copy(0, 1, 1, outward)
    mail_relay = [
        mail_copy(1, 3, 2, inward),
        mail_copy(2, 2, 3, outward),
        mail_copy(3, 3, 4, outward),
    ]

    other = (tp + 1) % n_tp
    theirs = pl.multiple_of(other * tokens, tokens)
    mine_at = pl.multiple_of(tp * tokens, tokens)
    act_copy = remote(
        act.at[pl.ds(theirs, tokens)], act_recv, act_sem.at[0], act_sem.at[1], (sp, other)
    )
    lot = tokens // CHUNK
    late = lot + 2

    first = plane * per
    tri_r = lax.broadcasted_iota(jnp.int32, (tokens, tokens), 0)
    tri_c = lax.broadcasted_iota(jnp.int32, (tokens, tokens), 1)
    later = (tri_r < tri_c).astype(F32).astype(BF16)
    spread_t = (
        (
            lax.broadcasted_iota(jnp.int32, (slots, per), 0) // capacity
            == lax.broadcasted_iota(jnp.int32, (slots, per), 1)
        )
        .astype(F32)
        .astype(BF16)
    )
    row_slot = (lax.broadcasted_iota(jnp.int32, (slots, tokens), 0) % capacity).astype(F32)
    row_expert = (
        first + lax.broadcasted_iota(jnp.int32, (slots, tokens), 0) // capacity
    ).astype(F32)
    expert_row = (first + lax.broadcasted_iota(jnp.int32, (per, tokens), 0)).astype(F32)

    def tables(b):
        routes, weight = mail[b, 0:2, :], mail[b, 2:4, :]
        member = (
            (routes[0:1, :] == expert_row).astype(F32)
            + (routes[1:2, :] == expert_row).astype(F32)
        ).astype(BF16)
        slot = jnp.dot(member, later, preferred_element_type=F32).astype(BF16)
        right = jnp.dot(spread_t, slot, preferred_element_type=F32) == row_slot
        hit0 = jnp.where(right & (routes[0:1, :] == row_expert), 1.0, 0.0)
        hit1 = jnp.where(right & (routes[1:2, :] == row_expert), 1.0, 0.0)
        picks[b] = (hit0 + hit1).astype(BF16)
        mix = (hit0 * weight[0:1, :] + hit1 * weight[1:2, :]).T
        high = mix.astype(BF16)
        highs[b] = high
        lows[b] = (mix - high.astype(F32)).astype(BF16)

    def conv_step(i, carry):
        @pl.when(i == 0)
        def _():
            pl.semaphore_wait(barrier, per - 1 + 1 + inner_count + has_next + has_last)

            @pl.when(sp < n_sp - 1)
            def _():
                for copy in halo_copies:
                    copy.start()

            @pl.when(edge)
            def _():
                mail_edge.start()

            @pl.when(inner)
            def _():
                mail_in.start()
                mail_out.start()

        @pl.when(i == late)
        def _():
            tables(0)

            @pl.when(sp > 0)
            def _():
                for copy in halo_copies:
                    copy.wait_recv()
                for g in range(groups):
                    glu_ext[g, pl.ds(0, HALO), :] = halo_recv[
                        :, g * group : (g + 1) * group
                    ].astype(F32)

        low = (
            (1 - i // lot) * (i + lot)
            + (i // lot) * (1 - i // late) * (i - lot + 1)
            + (i // (late + 1)) * (i - lot)
        )
        high = (1 - i // late) * (i + 1) + (i // (late + 1)) * i
        r = pl.multiple_of(((1 - tp) * low + tp * high) * CHUNK, CHUNK)
        mine = ids_here[pl.ds(r, CHUNK), :]
        sums = [jnp.zeros((CHUNK, group), F32) for _ in range(groups)]
        for tap in range(width):
            off = HALO - width + 1 + tap
            same = ids_ext[pl.ds(r + off, CHUNK), :] == mine
            for g in range(groups):
                term = (
                    tap_rows[tap : tap + 1, g * group : (g + 1) * group]
                    * glu_ext[g, pl.ds(r + off, CHUNK), :]
                )
                sums[g] = sums[g] + jnp.where(same, term, 0.0)
        for g in range(groups):
            at = slice(g * group, (g + 1) * group)
            centered = sums[g] - jnp.mean(sums[g], axis=-1, keepdims=True)
            var = jnp.mean(centered * centered, axis=-1, keepdims=True)
            v = centered * lax.rsqrt(var + epsilon) * gain_ref[:, at] + shift_ref[:, at]
            act[pl.ds(r, CHUNK), at] = silu(v).astype(BF16)

        @pl.when((i == lot - 1) & (tp == 0))
        def _():
            act_copy.start()

        @pl.when((i == late) & (tp == 1))
        def _():
            act_copy.start()

        return carry

    lax.fori_loop(0, rows // CHUNK, conv_step, 0)

    @pl.when(inner)
    def _():
        mail_copy(1, 1, 0, inward).wait_recv()
        mail_relay[0].start()
        mail_copy(2, 2, 0, inward).wait_recv()
        mail_relay[1].start()

    loads[10].wait()
    projected = jnp.dot(
        act[pl.ds(mine_at, tokens), :],
        conv_out[pl.ds(pl.multiple_of(tp * channels, channels), channels), :],
        preferred_element_type=F32,
    )
    act_copy.wait_recv()
    projected = projected + jnp.dot(
        act_recv[...],
        conv_out[pl.ds(pl.multiple_of(other * channels, channels), channels), :],
        preferred_element_type=F32,
    )
    stream = (resid_ref[...].astype(F32) + projected).astype(BF16).astype(F32)
    normed = (
        stream
        * lax.rsqrt(jnp.mean(stream * stream, axis=-1, keepdims=True) + epsilon)
        * ngain_ref[...]
    ).astype(BF16)
    for q in range(PARTS):
        tok[0, q] = normed[:, q * cols : (q + 1) * cols]
        base_ref[q] = stream[:, q * cols : (q + 1) * cols]

    def piece(index):
        return pl.ds(pl.multiple_of(index * capacity, capacity), capacity)

    chips = per // n_tp
    lane = chips * capacity
    chip = here // n_tp
    mine_row = tp * chips + chip

    def toward(sign):
        return place((plane + side * sign) * per + here)

    def tok_copy(sent, landed, index, q, where):
        return remote(
            tok.at[sent, q], tok.at[landed, q], tok_send.at[index, q], tok_recv.at[landed, q], where
        )

    def part_copy(b, landed, q, where):
        return remote(
            partial.at[b, q], inc.at[landed, q], part_send.at[b, q], part_recv.at[landed, q], where
        )

    def bytes_of(buffer, b, q, count, sem):
        area = buffer.at[b, q, pl.ds(0, count * capacity)]
        return remote(area, area, sem, sem, inward)

    def send_rows(core, b, q):
        for peer in peers:
            remote(
                outgoing.at[b, q, piece(peer)],
                arrived.at[b, q, piece(mine_row)],
                go_send.at[b, q],
                go_recv.at[b, q, core],
                peer_place(peer),
            ).start()
        arrived[b, q, piece(mine_row), :] = outgoing[b, q, piece(here), :]

    def return_rows(core, b, q, s):
        for apart in range(chips - 1, -1, -1):
            target = flip(chip, apart)
            if apart == 0 and s == core:
                returned[b, q, piece(here), :] = result[b, q, piece(mine_row), :]
            else:
                remote(
                    result.at[b, q, piece(s * chips + target)],
                    returned.at[b, q, piece(here)],
                    back_send.at[b, q],
                    back_recv.at[b, q],
                    peer_place(target * n_tp + s),
                ).start()

    landing = {"E": {0: (1, 1)}, "I": {0: (2, 1), 1: (1, -1)}}
    relaying = {1: (3, 2, 1), 2: (2, 3, -1), 3: (3, 4, -1)}
    part_to = {
        "E": {1: (0, 1), 2: (2, 1), 3: (3, 1)},
        "I": {1: (0, -1), 2: (1, 1), 3: (4, 1)},
    }
    joins = {1: 4, 2: 2, 3: 3}
    closes = {"E": (0,), "I": (0, 1)}

    def op(role, core, kind, b, q):
        if kind == "D":
            landed, sign = landing[role][b]
            tok_copy(0, landed, b, q, toward(sign)).start()
        elif kind == "T":
            if role == "E":
                mail_copy(b, b, 0, inward).wait_recv()
            tables(b)
        elif kind == "R":
            mail_copy(3, 3, 0, inward).wait_recv()
            mail_relay[2].start()
        elif kind == "L":
            tok_copy(b, b, 0, q, inward).wait_recv()
            landed, index, sign = relaying[b]
            tok_copy(b, landed, index, q, toward(sign)).start()
        elif kind == "P":
            if role == "E" and b:
                tok_copy(b, b, 0, q, inward).wait_recv()
            outgoing[b, q] = jnp.dot(picks[b], tok[b, q], preferred_element_type=F32).astype(BF16)
            send_rows(core, b, q)
        elif kind == "S":
            gate = jnp.zeros((tokens, sg.shape[1]), F32)
            up = jnp.zeros((tokens, sg.shape[1]), F32)
            for p in range(PARTS):
                k = slice(p * cols, (p + 1) * cols)
                gate = gate + jnp.dot(tok[0, p], sg[k, :], preferred_element_type=F32)
                up = up + jnp.dot(tok[0, p], su[k, :], preferred_element_type=F32)
            hidden = (silu(gate) * up).astype(BF16)
            for p in range(PARTS):
                k = slice(p * cols, (p + 1) * cols)
                base_ref[p] += jnp.dot(hidden, sd[:, k], preferred_element_type=F32)
        elif kind == "X":
            s, at = q, slice(q * lane, (q + 1) * lane)
            count = chips - int(s == core)
            gate_acc[...] = jnp.zeros((lane, eg.shape[2]), F32)
            up_acc[...] = jnp.zeros((lane, eg.shape[2]), F32)

            def widen(p, carry):
                k = pl.ds(pl.multiple_of(p * cols, cols), cols)
                bytes_of(arrived, b, p, count, go_recv.at[b, p, s]).wait_recv()
                x = arrived[b, p, at, :]
                gate_acc[...] += jnp.dot(x, eg[0, k, :], preferred_element_type=F32)
                up_acc[...] += jnp.dot(x, eu[0, k, :], preferred_element_type=F32)
                return carry

            lax.fori_loop(0, PARTS, widen, 0, unroll=2)
            hidden_ref[...] = (silu(gate_acc[...]) * up_acc[...]).astype(BF16)

            def narrow(p, carry):
                k = pl.ds(pl.multiple_of(p * cols, cols), cols)
                result[b, p, at, :] = jnp.dot(
                    hidden_ref[...], ed[0, :, k], preferred_element_type=F32
                ).astype(BF16)
                return_rows(core, b, p, s)
                return carry

            lax.fori_loop(0, PARTS, narrow, 0, unroll=2)
        elif kind == "M":
            bytes_of(returned, b, q, per - 1, back_recv.at[b, q]).wait_recv()
            back = returned[b, q]
            mixed = jnp.dot(highs[b], back, preferred_element_type=F32) + jnp.dot(
                lows[b], back, preferred_element_type=F32
            )
            if b == 0:
                base_ref[q] += mixed
                return
            if role == "I":
                joined = joins[b]
                part_copy(b, joined, q, inward).wait_recv()
                mixed = mixed + inc[joined, q].astype(F32)
            partial[b, q] = mixed.astype(BF16)
            landed, sign = part_to[role][b]
            part_copy(b, landed, q, toward(sign)).start()
        elif kind == "F":
            total = base_ref[q]
            for joined in closes[role]:
                part_copy(1, joined, q, inward).wait_recv()
                total = total + inc[joined, q].astype(F32)
            out_ref[:, q * cols : (q + 1) * cols] = total.astype(BF16)

    def close(role):
        for index, (landed, sign) in landing[role].items():
            for q in range(PARTS):
                tok_copy(0, landed, index, q, toward(sign)).wait_send()
        for b, (landed, index, sign) in relaying.items():
            if role == "I":
                for q in range(PARTS):
                    tok_copy(b, landed, index, q, toward(sign)).wait_send()
        for b, (landed, sign) in part_to[role].items():
            for q in range(PARTS):
                part_copy(b, landed, q, toward(sign)).wait_send()

    for load in loads[11:]:
        load.wait()
    for core in range(n_tp):
        for role, chosen in (("E", edge), ("I", inner)):

            @pl.when(chosen & (tp == core))
            def _(role=role, core=core):
                for step in ORDERS[role][core]:
                    op(role, core, step[0], int(step[1]), int(step[2]))
                close(role)

    @pl.when(edge)
    def _():
        mail_edge.wait_send()

    @pl.when(inner)
    def _():
        mail_in.wait_send()
        mail_out.wait_send()
        for copy in mail_relay:
            copy.wait_send()

    act_copy.wait_send()

    @pl.when(sp < n_sp - 1)
    def _():
        for copy in halo_copies:
            copy.wait_send()

    for b in range(PLANES):
        for q in range(PARTS):
            bytes_of(outgoing, b, q, per - 1, go_send.at[b, q]).wait_send()
            bytes_of(result, b, q, per - 1, back_send.at[b, q]).wait_send()


def fused(
    conv_value,
    conv_gate,
    taps,
    doc_ids,
    gn_gain,
    gn_shift,
    conv_out,
    residual,
    norm_gain,
    routes,
    route_weight,
    expert_gate,
    expert_up,
    expert_down,
    shared_gate,
    shared_up,
    shared_down,
):
    n_sp, n_tp = lax.axis_size("sp"), lax.axis_size("tp")
    n = n_sp * n_tp
    rows, channels = conv_value.shape
    tokens, model = residual.shape
    capacity = 2 * tokens * routes.shape[1] // n
    group = channels * n_tp // GROUPS
    slots = n // PLANES * capacity
    cols = model // PARTS
    operands = (
        conv_value,
        conv_gate,
        taps,
        doc_ids[None, :],
        gn_gain[None, :],
        gn_shift[None, :],
        residual,
        norm_gain[None, :],
        routes.T,
        route_weight.T,
        conv_out,
        shared_gate,
        shared_up,
        shared_down,
        expert_gate,
        expert_up,
        expert_down,
    )
    hbm = pl.BlockSpec(memory_space=pl.ANY)
    dma = pltpu.SemaphoreType.DMA
    return pl.pallas_call(
        functools.partial(fused_kernel, n_sp, n_tp, capacity),
        out_shape=pltpu.VMEM((tokens, model), BF16),
        in_specs=[hbm] * len(operands),
        out_specs=pl.BlockSpec(memory_space=pltpu.VMEM),
        scratch_shapes=[pltpu.VMEM(x.shape, x.dtype) for x in operands]
        + [
            pltpu.VMEM((channels // group, rows + HALO, group), F32),
            pltpu.VMEM((rows + HALO, group), F32),
            pltpu.VMEM((taps.shape[0] + 1, channels), F32),
            pltpu.VMEM((HALO, channels), BF16),
            pltpu.VMEM((HALO, channels), BF16),
            pltpu.VMEM((rows, channels), BF16),
            pltpu.VMEM((tokens, channels), BF16),
            pltpu.VMEM((rows, group), F32),
            pltpu.VMEM((PARTS, tokens, cols), F32),
            pltpu.VMEM((PLANES, 4, tokens), F32),
            pltpu.VMEM((PLANES, slots, tokens), BF16),
            pltpu.VMEM((PLANES, tokens, slots), BF16),
            pltpu.VMEM((PLANES, tokens, slots), BF16),
            pltpu.VMEM((PLANES, PARTS, tokens, cols), BF16),
            pltpu.VMEM((PLANES, PARTS, slots, cols), BF16),
            pltpu.VMEM((PLANES, PARTS, slots, cols), BF16),
            pltpu.VMEM((PLANES, PARTS, slots, cols), BF16),
            pltpu.VMEM((PLANES, PARTS, slots, cols), BF16),
            pltpu.VMEM((PLANES, PARTS, tokens, cols), BF16),
            pltpu.VMEM((5, PARTS, tokens, cols), BF16),
            pltpu.VMEM((slots // n_tp, expert_gate.shape[2]), F32),
            pltpu.VMEM((slots // n_tp, expert_gate.shape[2]), F32),
            pltpu.VMEM((slots // n_tp, expert_gate.shape[2]), BF16),
            dma((17,)),
            dma((4,)),
            dma((2,)),
            dma((5,)),
            dma((PLANES,)),
            dma((5, PARTS)),
            dma((PLANES, PARTS)),
            dma((PLANES, PARTS)),
            dma((PLANES, PARTS, n_tp)),
            dma((PLANES, PARTS)),
            dma((PLANES, PARTS)),
            dma((PLANES, PARTS)),
            dma((5, PARTS)),
        ],
        compiler_params=pltpu.CompilerParams(
            collective_id=0, has_side_effects=True, vmem_limit_bytes=VMEM_LIMIT
        ),
    )(*operands)


def fits(mesh):
    n = mesh.size
    return n & (n - 1) == 0 and 8 < n <= 32 and mesh.shape["tp"] == 2


def solution(mesh):
    return jax.shard_map(
        fused if fits(mesh) else per_device,
        mesh=mesh,
        in_specs=(
            P("sp", "tp"),
            P("sp", "tp"),
            P(None, "tp"),
            P("sp"),
            P("tp"),
            P("tp"),
            P(),
            P(("sp", "tp"), None),
            P(),
            P(("sp", "tp"), None),
            P(("sp", "tp"), None),
            P(("sp", "tp"), None, None),
            P(("sp", "tp"), None, None),
            P(("sp", "tp"), None, None),
            P(),
            P(),
            P(),
        ),
        out_specs=P(("sp", "tp"), None),
        check_vma=False,
    )
```

```python
import functools

import jax
import jax.numpy as jnp
from jax import lax
from jax.experimental import pallas as pl
from jax.experimental.pallas import tpu as pltpu
from jax.sharding import PartitionSpec as P

GROUPS = 8


epsilon = 1e-06


def from_behind(x, axis, by):
    peers = lax.axis_size(axis)
    pairs = [(i, i + by) for i in range(peers) if 0 <= i + by < peers]
    return lax.ppermute(x, axis, pairs)


def per_device(
    conv_value,
    conv_gate,
    taps,
    doc_ids,
    gn_gain,
    gn_shift,
    conv_out,
    residual,
    norm_gain,
    routes,
    route_weight,
    expert_gate,
    expert_up,
    expert_down,
    shared_gate,
    shared_up,
    shared_down,
):
    position_count, channel_count = conv_value.shape
    kernel_width = taps.shape[0]
    model_width = residual.shape[1]
    glu_out = (
        conv_value.astype(jnp.float32) * jax.nn.sigmoid(conv_gate.astype(jnp.float32))
    ).astype(jnp.bfloat16)
    rim_start = position_count - kernel_width + 1
    edge_glu, edge_ids = from_behind((glu_out[rim_start:], doc_ids[rim_start:]), "sp", 1)
    longer_glu = jnp.concatenate([edge_glu, glu_out], axis=0)
    longer_ids = jnp.concatenate([edge_ids, doc_ids], axis=0)
    conv_sum = jnp.zeros((position_count, channel_count), jnp.float32)
    for offset in range(kernel_width):
        same_doc = (longer_ids[offset : offset + position_count] == doc_ids)[:, None]
        tap_term = taps[offset].astype(jnp.float32)[None, :] * longer_glu[
            offset : offset + position_count
        ].astype(jnp.float32)
        conv_sum = conv_sum + jnp.where(same_doc, tap_term, 0.0)
    core_split = lax.axis_size("tp")
    groups_here = GROUPS // core_split
    grouped = conv_sum.reshape(position_count, groups_here, channel_count // groups_here)
    group_mean = jnp.mean(grouped, axis=-1, keepdims=True)
    centered = grouped - group_mean
    group_var = jnp.mean(centered * centered, axis=-1, keepdims=True)
    normalized = (centered * lax.rsqrt(group_var + epsilon)).reshape(position_count, channel_count)
    conv_act = jax.nn.silu(normalized * gn_gain + gn_shift).astype(jnp.bfloat16)
    token_rows = lax.all_to_all(conv_act, "tp", split_axis=0, concat_axis=1, tiled=True)
    projected = jnp.dot(token_rows, conv_out, preferred_element_type=jnp.float32)
    stream = (residual.astype(jnp.float32) + projected).astype(jnp.bfloat16)
    stream_wide = stream.astype(jnp.float32)
    normed = (
        stream_wide
        * lax.rsqrt(jnp.mean(stream_wide * stream_wide, axis=-1, keepdims=True) + epsilon)
        * norm_gain
    ).astype(jnp.bfloat16)
    token_count, top_count = routes.shape
    sequence_split = lax.axis_size("sp")
    device_count = sequence_split * core_split
    local_experts = expert_gate.shape[0]
    experts = local_experts * device_count
    capacity = 2 * token_count * top_count // experts
    flat_routes = routes.reshape(-1)
    onehot = (flat_routes[:, None] == jnp.arange(experts, dtype=jnp.int32)[None, :]).astype(
        jnp.int32
    )
    slot_index = jnp.sum(jnp.cumsum(onehot, axis=0) * onehot, axis=1) - 1
    target = flat_routes * capacity + slot_index
    source = (
        jnp.full((experts * capacity,), token_count, jnp.int32)
        .at[target]
        .set(jnp.arange(token_count * top_count, dtype=jnp.int32) // top_count)
    )
    padded_rows = jnp.concatenate([normed, jnp.zeros((1, model_width), normed.dtype)], axis=0)
    outgoing = padded_rows[source]
    shared_hidden = (
        jax.nn.silu(jnp.dot(normed, shared_gate, preferred_element_type=jnp.float32))
        * jnp.dot(normed, shared_up, preferred_element_type=jnp.float32)
    ).astype(jnp.bfloat16)
    shared_out = jnp.dot(shared_hidden, shared_down, preferred_element_type=jnp.float32)
    parcel = outgoing.reshape(device_count, local_experts, capacity, model_width)
    arrived = lax.all_to_all(parcel, ("sp", "tp"), split_axis=0, concat_axis=0, tiled=True)
    expert_rows = arrived[:, 0].reshape(-1, model_width)
    gate_part = jnp.dot(expert_rows, expert_gate[0], preferred_element_type=jnp.float32)
    up_part = jnp.dot(expert_rows, expert_up[0], preferred_element_type=jnp.float32)
    hidden = (jax.nn.silu(gate_part) * up_part).astype(jnp.bfloat16)
    result = jnp.dot(hidden, expert_down[0], preferred_element_type=jnp.float32).astype(
        jnp.bfloat16
    )
    results = [result.reshape(arrived.shape[0], arrived.shape[2], model_width)]
    returned = lax.all_to_all(
        jnp.stack(results, axis=1), ("sp", "tp"), split_axis=0, concat_axis=0, tiled=True
    )
    picked = returned.reshape(experts * capacity, model_width)[target].reshape(
        token_count, top_count, model_width
    )
    routed = jnp.zeros((token_count, model_width), jnp.float32)
    for route_index in range(top_count):
        routed = routed + route_weight[:, route_index, None] * picked[:, route_index].astype(
            jnp.float32
        )
    return (stream_wide + shared_out + routed).astype(jnp.bfloat16)


F32 = jnp.float32
BF16 = jnp.bfloat16
MESH_ID = pl.DeviceIdType.MESH
HALO = 32
CHUNK = 32
PLANES = 4
PARTS = 4
VMEM_LIMIT = 58 * 1024 * 1024


def flip(index, bits):
    out, weight = index, 1
    while weight <= bits:
        if (bits // weight) % 2:
            out = out + weight * (1 - 2 * ((index // weight) % 2))
        weight *= 2
    return out


def silu(v):
    return v / (1.0 + jnp.exp(-v))


ORDERS = {
    "E": (
        (
            "D00", "T20", "P03", "P02", "P00", "X01", "D02", "D03", "D01", "P01", "X11", "T30",
            "X21", "S00", "P32", "P22", "P31", "T10", "P30", "P33", "X31", "P21", "P20", "P23",
            "X30", "P12", "P10", "P11", "M31", "M33", "M32", "P13", "X20", "X00", "M30", "M20",
            "M21", "X10", "M23", "M22", "M01", "M02", "M10", "F01", "M03", "M00", "M13", "F03",
            "M12", "M11", "F02", "F00",
        ),
        (
            "P02", "P03", "P00", "D03", "D01", "D00", "P01", "T20", "T10", "D02", "P10", "P13",
            "P12", "P11", "P22", "P20", "T30", "P21", "P23", "X01", "P33", "X21", "X11", "M02",
            "P30", "M01", "M03", "M20", "P32", "P31", "M22", "M21", "M12", "M11", "M23", "M13",
            "X31", "M30", "M31", "X30", "M32", "S00", "M33", "X00", "X20", "M10", "X10", "M00",
            "F00", "F01", "F02", "F03",
        ),
    ),
    "I": (
        (
            "P02", "P03", "P01", "T10", "L10", "P00", "R00", "T20", "L12", "T30", "P12", "D02",
            "X00", "L11", "L30", "S00", "L13", "L22", "L32", "D03", "L31", "D01", "L33", "P13",
            "D00", "X01", "P31", "M02", "L21", "L23", "M00", "X21", "L20", "D10", "P11", "D13",
            "P33", "D12", "P32", "D11", "X31", "P30", "P22", "X11", "P20", "P10", "P23", "P21",
            "X30", "X10", "M31", "X20", "M33", "M32", "M11", "M01", "M30", "M13", "M20", "M12",
            "M21", "M10", "M23", "M22", "F00", "F02", "M03", "F03", "F01",
        ),
        (
            "D12", "D10", "D13", "D00", "T10", "D02", "D01", "T20", "D03", "S00", "D11", "P02",
            "P03", "L20", "P00", "P01", "P20", "L22", "L21", "L13", "R00", "P21", "T30", "P13",
            "L10", "L23", "P22", "L11", "P10", "P23", "L12", "L33", "P33", "P11", "X00", "L30",
            "P30", "L31", "P12", "P31", "X21", "L32", "P32", "X01", "X11", "M01", "M02", "X31",
            "M20", "M03", "M22", "M23", "M21", "M30", "M31", "X30", "M32", "M00", "F03", "F02",
            "M10", "F01", "M33", "M11", "X10", "M12", "X20", "M13", "F00",
        ),
    ),
}


def fused_kernel(n_sp, n_tp, capacity, *refs):
    hbm_in, out_ref = refs[:17], refs[17]
    vmem_in = refs[18:35]
    (
        glu_ext,
        ids_ext,
        tap_rows,
        halo_send,
        halo_recv,
        act,
        act_recv,
        ids_here,
        base_ref,
        mail,
        picks,
        highs,
        lows,
        tok,
        outgoing,
        arrived,
        result,
        returned,
        partial,
        inc,
        gate_acc,
        up_acc,
        hidden_ref,
        load_sem,
        halo_sem,
        act_sem,
        mail_send,
        mail_recv,
        tok_send,
        tok_recv,
        go_send,
        go_recv,
        back_send,
        back_recv,
        part_send,
        part_recv,
    ) = refs[35:]
    (
        value_ref,
        gate_ref,
        taps_ref,
        ids_ref,
        gain_ref,
        shift_ref,
        resid_ref,
        ngain_ref,
        routes_ref,
        weight_ref,
        conv_out,
        sg,
        su,
        sd,
        eg,
        eu,
        ed,
    ) = vmem_in
    n = n_sp * n_tp
    per = n // PLANES
    sp, tp = lax.axis_index("sp"), lax.axis_index("tp")
    me = sp * n_tp + tp
    plane, here = me // per, me % per
    rows, channels = value_ref.shape
    tokens, model = resid_ref.shape
    width = taps_ref.shape[0]
    group = glu_ext.shape[2]
    groups = channels // group
    cols = model // PARTS
    slots = per * capacity
    side = 1 - 2 * (plane // 2)
    edge = plane % (PLANES - 1) == 0
    inner = plane % (PLANES - 1) != 0
    inner_count = (plane % (PLANES - 1) + 1) // 2

    def place(index):
        return (index // n_tp, index % n_tp)

    inward = place((plane + side) * per + here)
    outward = place((plane - side) * per + here)
    peers = [flip(here, k) for k in range(per - 1, 0, -1)]

    def peer_place(peer):
        return place(plane * per + peer)

    loads = [
        pltpu.make_async_copy(a, b, load_sem.at[i])
        for i, (a, b) in enumerate(zip(hbm_in, vmem_in))
    ]
    barrier = pltpu.get_barrier_semaphore()

    def greet(where):
        pl.semaphore_signal(barrier, inc=1, device_id=where, device_id_type=MESH_ID)

    for load in loads:
        load.start()
    for peer in peers:
        greet(peer_place(peer))
    greet(inward)

    @pl.when(inner)
    def _():
        greet(outward)

    @pl.when(sp < n_sp - 1)
    def _():
        greet((sp + 1, tp))

    @pl.when(sp > 0)
    def _():
        greet((sp - 1, tp))

    has_next = 1 - (sp + 1) // n_sp
    has_last = (sp + n_sp - 1) // n_sp
    for load in loads[:10]:
        load.wait()

    mail[0, 0:2, :] = routes_ref[...].astype(F32)
    mail[0, 2:4, :] = weight_ref[...]
    glu = (value_ref[...].astype(F32) * jax.nn.sigmoid(gate_ref[...].astype(F32))).astype(BF16)
    halo_send[...] = glu[rows - HALO :, :]
    for g in range(groups):
        glu_ext[g, pl.ds(HALO, rows), :] = glu[:, g * group : (g + 1) * group].astype(F32)
    for at in range(0, rows, group):
        row = ids_ref[:, at : at + group].astype(F32)
        column = jnp.broadcast_to(row, (group, group)).T
        ids_here[pl.ds(at, group), :] = column
        ids_ext[pl.ds(HALO + at, group), :] = column
    tap_rows[pl.ds(0, width), :] = taps_ref[...].astype(F32)

    def remote(src, dst, send_sem, recv_sem, where):
        return pltpu.make_async_remote_copy(
            src_ref=src,
            dst_ref=dst,
            send_sem=send_sem,
            recv_sem=recv_sem,
            device_id=where,
            device_id_type=MESH_ID,
        )

    halo_copies = [
        remote(halo_send, halo_recv, halo_sem.at[0], halo_sem.at[1], (sp + 1, tp)),
        remote(
            ids_here.at[pl.ds(rows - HALO, HALO)],
            ids_ext.at[pl.ds(0, HALO)],
            halo_sem.at[2],
            halo_sem.at[3],
            (sp + 1, tp),
        ),
    ]

    @pl.when(sp == 0)
    def _():
        glu_ext[:, pl.ds(0, HALO), :] = jnp.zeros((groups, HALO, group), F32)
        ids_ext[pl.ds(0, HALO), :] = jnp.full((HALO, group), -1.0, F32)

    def mail_copy(sent, landed, index, where):
        return remote(
            mail.at[sent], mail.at[landed], mail_send.at[index], mail_recv.at[landed], where
        )

    mail_edge = mail_copy(0, 1, 0, inward)
    mail_in = mail_copy(0, 2, 0, inward)
    mail_out = mail_copy(0, 1, 1, outward)
    mail_relay = [
        mail_copy(1, 3, 2, inward),
        mail_copy(2, 2, 3, outward),
        mail_copy(3, 3, 4, outward),
    ]

    other = (tp + 1) % n_tp
    theirs = pl.multiple_of(other * tokens, tokens)
    mine_at = pl.multiple_of(tp * tokens, tokens)
    act_copy = remote(
        act.at[pl.ds(theirs, tokens)], act_recv, act_sem.at[0], act_sem.at[1], (sp, other)
    )
    lot = tokens // CHUNK
    late = lot + 2

    first = plane * per
    tri_r = lax.broadcasted_iota(jnp.int32, (tokens, tokens), 0)
    tri_c = lax.broadcasted_iota(jnp.int32, (tokens, tokens), 1)
    later = (tri_r < tri_c).astype(F32).astype(BF16)
    spread_t = (
        (
            lax.broadcasted_iota(jnp.int32, (slots, per), 0) // capacity
            == lax.broadcasted_iota(jnp.int32, (slots, per), 1)
        )
        .astype(F32)
        .astype(BF16)
    )
    row_slot = (lax.broadcasted_iota(jnp.int32, (slots, tokens), 0) % capacity).astype(F32)
    row_expert = (
        first + lax.broadcasted_iota(jnp.int32, (slots, tokens), 0) // capacity
    ).astype(F32)
    expert_row = (first + lax.broadcasted_iota(jnp.int32, (per, tokens), 0)).astype(F32)

    def tables(b):
        routes, weight = mail[b, 0:2, :], mail[b, 2:4, :]
        member = (
            (routes[0:1, :] == expert_row).astype(F32)
            + (routes[1:2, :] == expert_row).astype(F32)
        ).astype(BF16)
        slot = jnp.dot(member, later, preferred_element_type=F32).astype(BF16)
        right = jnp.dot(spread_t, slot, preferred_element_type=F32) == row_slot
        hit0 = jnp.where(right & (routes[0:1, :] == row_expert), 1.0, 0.0)
        hit1 = jnp.where(right & (routes[1:2, :] == row_expert), 1.0, 0.0)
        picks[b] = (hit0 + hit1).astype(BF16)
        mix = (hit0 * weight[0:1, :] + hit1 * weight[1:2, :]).T
        high = mix.astype(BF16)
        highs[b] = high
        lows[b] = (mix - high.astype(F32)).astype(BF16)

    def conv_step(i, carry):
        @pl.when(i == 0)
        def _():
            pl.semaphore_wait(barrier, per - 1 + 1 + inner_count + has_next + has_last)

            @pl.when(sp < n_sp - 1)
            def _():
                for copy in halo_copies:
                    copy.start()

            @pl.when(edge)
            def _():
                mail_edge.start()

            @pl.when(inner)
            def _():
                mail_in.start()
                mail_out.start()

        @pl.when(i == late)
        def _():
            tables(0)

            @pl.when(sp > 0)
            def _():
                for copy in halo_copies:
                    copy.wait_recv()
                for g in range(groups):
                    glu_ext[g, pl.ds(0, HALO), :] = halo_recv[
                        :, g * group : (g + 1) * group
                    ].astype(F32)

        low = (
            (1 - i // lot) * (i + lot)
            + (i // lot) * (1 - i // late) * (i - lot + 1)
            + (i // (late + 1)) * (i - lot)
        )
        high = (1 - i // late) * (i + 1) + (i // (late + 1)) * i
        r = pl.multiple_of(((1 - tp) * low + tp * high) * CHUNK, CHUNK)
        mine = ids_here[pl.ds(r, CHUNK), :]
        sums = [jnp.zeros((CHUNK, group), F32) for _ in range(groups)]
        for tap in range(width):
            off = HALO - width + 1 + tap
            same = ids_ext[pl.ds(r + off, CHUNK), :] == mine
            for g in range(groups):
                term = (
                    tap_rows[tap : tap + 1, g * group : (g + 1) * group]
                    * glu_ext[g, pl.ds(r + off, CHUNK), :]
                )
                sums[g] = sums[g] + jnp.where(same, term, 0.0)
        for g in range(groups):
            at = slice(g * group, (g + 1) * group)
            centered = sums[g] - jnp.mean(sums[g], axis=-1, keepdims=True)
            var = jnp.mean(centered * centered, axis=-1, keepdims=True)
            v = centered * lax.rsqrt(var + epsilon) * gain_ref[:, at] + shift_ref[:, at]
            act[pl.ds(r, CHUNK), at] = silu(v).astype(BF16)

        @pl.when((i == lot - 1) & (tp == 0))
        def _():
            act_copy.start()

        @pl.when((i == late) & (tp == 1))
        def _():
            act_copy.start()

        return carry

    lax.fori_loop(0, rows // CHUNK, conv_step, 0)

    @pl.when(inner)
    def _():
        mail_copy(1, 1, 0, inward).wait_recv()
        mail_relay[0].start()
        mail_copy(2, 2, 0, inward).wait_recv()
        mail_relay[1].start()

    loads[10].wait()
    projected = jnp.dot(
        act[pl.ds(mine_at, tokens), :],
        conv_out[pl.ds(pl.multiple_of(tp * channels, channels), channels), :],
        preferred_element_type=F32,
    )
    act_copy.wait_recv()
    projected = projected + jnp.dot(
        act_recv[...],
        conv_out[pl.ds(pl.multiple_of(other * channels, channels), channels), :],
        preferred_element_type=F32,
    )
    stream = (resid_ref[...].astype(F32) + projected).astype(BF16).astype(F32)
    normed = (
        stream
        * lax.rsqrt(jnp.mean(stream * stream, axis=-1, keepdims=True) + epsilon)
        * ngain_ref[...]
    ).astype(BF16)
    for q in range(PARTS):
        tok[0, q] = normed[:, q * cols : (q + 1) * cols]
        base_ref[q] = stream[:, q * cols : (q + 1) * cols]

    def piece(index):
        return pl.ds(pl.multiple_of(index * capacity, capacity), capacity)

    chips = per // n_tp
    lane = chips * capacity
    chip = here // n_tp
    mine_row = tp * chips + chip

    def toward(sign):
        return place((plane + side * sign) * per + here)

    def tok_copy(sent, landed, index, q, where):
        return remote(
            tok.at[sent, q], tok.at[landed, q], tok_send.at[index, q], tok_recv.at[landed, q], where
        )

    def part_copy(b, landed, q, where):
        return remote(
            partial.at[b, q], inc.at[landed, q], part_send.at[b, q], part_recv.at[landed, q], where
        )

    def bytes_of(buffer, b, q, count, sem):
        area = buffer.at[b, q, pl.ds(0, count * capacity)]
        return remote(area, area, sem, sem, inward)

    def send_rows(core, b, q):
        for peer in peers:
            remote(
                outgoing.at[b, q, piece(peer)],
                arrived.at[b, q, piece(mine_row)],
                go_send.at[b, q],
                go_recv.at[b, q, core],
                peer_place(peer),
            ).start()
        arrived[b, q, piece(mine_row), :] = outgoing[b, q, piece(here), :]

    def return_rows(core, b, q, s):
        for apart in range(chips - 1, -1, -1):
            target = flip(chip, apart)
            if apart == 0 and s == core:
                returned[b, q, piece(here), :] = result[b, q, piece(mine_row), :]
            else:
                remote(
                    result.at[b, q, piece(s * chips + target)],
                    returned.at[b, q, piece(here)],
                    back_send.at[b, q],
                    back_recv.at[b, q],
                    peer_place(target * n_tp + s),
                ).start()

    landing = {"E": {0: (1, 1)}, "I": {0: (2, 1), 1: (1, -1)}}
    relaying = {1: (3, 2, 1), 2: (2, 3, -1), 3: (3, 4, -1)}
    part_to = {
        "E": {1: (0, 1), 2: (2, 1), 3: (3, 1)},
        "I": {1: (0, -1), 2: (1, 1), 3: (4, 1)},
    }
    joins = {1: 4, 2: 2, 3: 3}
    closes = {"E": (0,), "I": (0, 1)}

    def op(role, core, kind, b, q):
        if kind == "D":
            landed, sign = landing[role][b]
            tok_copy(0, landed, b, q, toward(sign)).start()
        elif kind == "T":
            if role == "E":
                mail_copy(b, b, 0, inward).wait_recv()
            tables(b)
        elif kind == "R":
            mail_copy(3, 3, 0, inward).wait_recv()
            mail_relay[2].start()
        elif kind == "L":
            tok_copy(b, b, 0, q, inward).wait_recv()
            landed, index, sign = relaying[b]
            tok_copy(b, landed, index, q, toward(sign)).start()
        elif kind == "P":
            if role == "E" and b:
                tok_copy(b, b, 0, q, inward).wait_recv()
            outgoing[b, q] = jnp.dot(picks[b], tok[b, q], preferred_element_type=F32).astype(BF16)
            send_rows(core, b, q)
        elif kind == "S":
            gate = jnp.zeros((tokens, sg.shape[1]), F32)
            up = jnp.zeros((tokens, sg.shape[1]), F32)
            for p in range(PARTS):
                k = slice(p * cols, (p + 1) * cols)
                gate = gate + jnp.dot(tok[0, p], sg[k, :], preferred_element_type=F32)
                up = up + jnp.dot(tok[0, p], su[k, :], preferred_element_type=F32)
            hidden = (silu(gate) * up).astype(BF16)
            for p in range(PARTS):
                k = slice(p * cols, (p + 1) * cols)
                base_ref[p] += jnp.dot(hidden, sd[:, k], preferred_element_type=F32)
        elif kind == "X":
            s, at = q, slice(q * lane, (q + 1) * lane)
            count = chips - int(s == core)
            gate_acc[...] = jnp.zeros((lane, eg.shape[2]), F32)
            up_acc[...] = jnp.zeros((lane, eg.shape[2]), F32)

            def widen(p, carry):
                k = pl.ds(pl.multiple_of(p * cols, cols), cols)
                bytes_of(arrived, b, p, count, go_recv.at[b, p, s]).wait_recv()
                x = arrived[b, p, at, :]
                gate_acc[...] += jnp.dot(x, eg[0, k, :], preferred_element_type=F32)
                up_acc[...] += jnp.dot(x, eu[0, k, :], preferred_element_type=F32)
                return carry

            lax.fori_loop(0, PARTS, widen, 0, unroll=2)
            hidden_ref[...] = (silu(gate_acc[...]) * up_acc[...]).astype(BF16)

            def narrow(p, carry):
                k = pl.ds(pl.multiple_of(p * cols, cols), cols)
                result[b, p, at, :] = jnp.dot(
                    hidden_ref[...], ed[0, :, k], preferred_element_type=F32
                ).astype(BF16)
                return_rows(core, b, p, s)
                return carry

            lax.fori_loop(0, PARTS, narrow, 0, unroll=2)
        elif kind == "M":
            bytes_of(returned, b, q, per - 1, back_recv.at[b, q]).wait_recv()
            back = returned[b, q]
            mixed = jnp.dot(highs[b], back, preferred_element_type=F32) + jnp.dot(
                lows[b], back, preferred_element_type=F32
            )
            if b == 0:
                base_ref[q] += mixed
                return
            if role == "I":
                joined = joins[b]
                part_copy(b, joined, q, inward).wait_recv()
                mixed = mixed + inc[joined, q].astype(F32)
            partial[b, q] = mixed.astype(BF16)
            landed, sign = part_to[role][b]
            part_copy(b, landed, q, toward(sign)).start()
        elif kind == "F":
            total = base_ref[q]
            for joined in closes[role]:
                part_copy(1, joined, q, inward).wait_recv()
                total = total + inc[joined, q].astype(F32)
            out_ref[:, q * cols : (q + 1) * cols] = total.astype(BF16)

    def close(role):
        for index, (landed, sign) in landing[role].items():
            for q in range(PARTS):
                tok_copy(0, landed, index, q, toward(sign)).wait_send()
        for b, (landed, index, sign) in relaying.items():
            if role == "I":
                for q in range(PARTS):
                    tok_copy(b, landed, index, q, toward(sign)).wait_send()
        for b, (landed, sign) in part_to[role].items():
            for q in range(PARTS):
                part_copy(b, landed, q, toward(sign)).wait_send()

    for load in loads[11:]:
        load.wait()
    for core in range(n_tp):
        for role, chosen in (("E", edge), ("I", inner)):

            @pl.when(chosen & (tp == core))
            def _(role=role, core=core):
                for step in ORDERS[role][core]:
                    op(role, core, step[0], int(step[1]), int(step[2]))
                close(role)

    @pl.when(edge)
    def _():
        mail_edge.wait_send()

    @pl.when(inner)
    def _():
        mail_in.wait_send()
        mail_out.wait_send()
        for copy in mail_relay:
            copy.wait_send()

    act_copy.wait_send()

    @pl.when(sp < n_sp - 1)
    def _():
        for copy in halo_copies:
            copy.wait_send()

    for b in range(PLANES):
        for q in range(PARTS):
            bytes_of(outgoing, b, q, per - 1, go_send.at[b, q]).wait_send()
            bytes_of(result, b, q, per - 1, back_send.at[b, q]).wait_send()


def fused(
    conv_value,
    conv_gate,
    taps,
    doc_ids,
    gn_gain,
    gn_shift,
    conv_out,
    residual,
    norm_gain,
    routes,
    route_weight,
    expert_gate,
    expert_up,
    expert_down,
    shared_gate,
    shared_up,
    shared_down,
):
    n_sp, n_tp = lax.axis_size("sp"), lax.axis_size("tp")
    n = n_sp * n_tp
    rows, channels = conv_value.shape
    tokens, model = residual.shape
    capacity = 2 * tokens * routes.shape[1] // n
    group = channels * n_tp // GROUPS
    slots = n // PLANES * capacity
    cols = model // PARTS
    operands = (
        conv_value,
        conv_gate,
        taps,
        doc_ids[None, :],
        gn_gain[None, :],
        gn_shift[None, :],
        residual,
        norm_gain[None, :],
        routes.T,
        route_weight.T,
        conv_out,
        shared_gate,
        shared_up,
        shared_down,
        expert_gate,
        expert_up,
        expert_down,
    )
    hbm = pl.BlockSpec(memory_space=pl.ANY)
    dma = pltpu.SemaphoreType.DMA
    return pl.pallas_call(
        functools.partial(fused_kernel, n_sp, n_tp, capacity),
        out_shape=pltpu.VMEM((tokens, model), BF16),
        in_specs=[hbm] * len(operands),
        out_specs=pl.BlockSpec(memory_space=pltpu.VMEM),
        scratch_shapes=[pltpu.VMEM(x.shape, x.dtype) for x in operands]
        + [
            pltpu.VMEM((channels // group, rows + HALO, group), F32),
            pltpu.VMEM((rows + HALO, group), F32),
            pltpu.VMEM((taps.shape[0] + 1, channels), F32),
            pltpu.VMEM((HALO, channels), BF16),
            pltpu.VMEM((HALO, channels), BF16),
            pltpu.VMEM((rows, channels), BF16),
            pltpu.VMEM((tokens, channels), BF16),
            pltpu.VMEM((rows, group), F32),
            pltpu.VMEM((PARTS, tokens, cols), F32),
            pltpu.VMEM((PLANES, 4, tokens), F32),
            pltpu.VMEM((PLANES, slots, tokens), BF16),
            pltpu.VMEM((PLANES, tokens, slots), BF16),
            pltpu.VMEM((PLANES, tokens, slots), BF16),
            pltpu.VMEM((PLANES, PARTS, tokens, cols), BF16),
            pltpu.VMEM((PLANES, PARTS, slots, cols), BF16),
            pltpu.VMEM((PLANES, PARTS, slots, cols), BF16),
            pltpu.VMEM((PLANES, PARTS, slots, cols), BF16),
            pltpu.VMEM((PLANES, PARTS, slots, cols), BF16),
            pltpu.VMEM((PLANES, PARTS, tokens, cols), BF16),
            pltpu.VMEM((5, PARTS, tokens, cols), BF16),
            pltpu.VMEM((slots // n_tp, expert_gate.shape[2]), F32),
            pltpu.VMEM((slots // n_tp, expert_gate.shape[2]), F32),
            pltpu.VMEM((slots // n_tp, expert_gate.shape[2]), BF16),
            dma((17,)),
            dma((4,)),
            dma((2,)),
            dma((5,)),
            dma((PLANES,)),
            dma((5, PARTS)),
            dma((PLANES, PARTS)),
            dma((PLANES, PARTS)),
            dma((PLANES, PARTS, n_tp)),
            dma((PLANES, PARTS)),
            dma((PLANES, PARTS)),
            dma((PLANES, PARTS)),
            dma((5, PARTS)),
        ],
        compiler_params=pltpu.CompilerParams(
            collective_id=0, has_side_effects=True, vmem_limit_bytes=VMEM_LIMIT
        ),
    )(*operands)


def fits(mesh):
    n = mesh.size
    return n & (n - 1) == 0 and 8 < n <= 32 and mesh.shape["tp"] == 2


def solution(mesh):
    return jax.shard_map(
        fused if fits(mesh) else per_device,
        mesh=mesh,
        in_specs=(
            P("sp", "tp"),
            P("sp", "tp"),
            P(None, "tp"),
            P("sp"),
            P("tp"),
            P("tp"),
            P(),
            P(("sp", "tp"), None),
            P(),
            P(("sp", "tp"), None),
            P(("sp", "tp"), None),
            P(("sp", "tp"), None, None),
            P(("sp", "tp"), None, None),
            P(("sp", "tp"), None, None),
            P(),
            P(),
            P(),
        ),
        out_specs=P(("sp", "tp"), None),
        check_vma=False,
    )
```

```python
import functools

import jax
import jax.numpy as jnp
from jax import lax
from jax.experimental import pallas as pl
from jax.experimental.pallas import tpu as pltpu
from jax.sharding import PartitionSpec as P

GROUPS = 8


epsilon = 1e-06


def from_behind(x, axis, by):
    peers = lax.axis_size(axis)
    pairs = [(i, i + by) for i in range(peers) if 0 <= i + by < peers]
    return lax.ppermute(x, axis, pairs)


def per_device(
    conv_value,
    conv_gate,
    taps,
    doc_ids,
    gn_gain,
    gn_shift,
    conv_out,
    residual,
    norm_gain,
    routes,
    route_weight,
    expert_gate,
    expert_up,
    expert_down,
    shared_gate,
    shared_up,
    shared_down,
):
    position_count, channel_count = conv_value.shape
    kernel_width = taps.shape[0]
    model_width = residual.shape[1]
    glu_out = (
        conv_value.astype(jnp.float32) * jax.nn.sigmoid(conv_gate.astype(jnp.float32))
    ).astype(jnp.bfloat16)
    rim_start = position_count - kernel_width + 1
    edge_glu, edge_ids = from_behind((glu_out[rim_start:], doc_ids[rim_start:]), "sp", 1)
    longer_glu = jnp.concatenate([edge_glu, glu_out], axis=0)
    longer_ids = jnp.concatenate([edge_ids, doc_ids], axis=0)
    conv_sum = jnp.zeros((position_count, channel_count), jnp.float32)
    for offset in range(kernel_width):
        same_doc = (longer_ids[offset : offset + position_count] == doc_ids)[:, None]
        tap_term = taps[offset].astype(jnp.float32)[None, :] * longer_glu[
            offset : offset + position_count
        ].astype(jnp.float32)
        conv_sum = conv_sum + jnp.where(same_doc, tap_term, 0.0)
    core_split = lax.axis_size("tp")
    groups_here = GROUPS // core_split
    grouped = conv_sum.reshape(position_count, groups_here, channel_count // groups_here)
    group_mean = jnp.mean(grouped, axis=-1, keepdims=True)
    centered = grouped - group_mean
    group_var = jnp.mean(centered * centered, axis=-1, keepdims=True)
    normalized = (centered * lax.rsqrt(group_var + epsilon)).reshape(position_count, channel_count)
    conv_act = jax.nn.silu(normalized * gn_gain + gn_shift).astype(jnp.bfloat16)
    token_rows = lax.all_to_all(conv_act, "tp", split_axis=0, concat_axis=1, tiled=True)
    projected = jnp.dot(token_rows, conv_out, preferred_element_type=jnp.float32)
    stream = (residual.astype(jnp.float32) + projected).astype(jnp.bfloat16)
    stream_wide = stream.astype(jnp.float32)
    normed = (
        stream_wide
        * lax.rsqrt(jnp.mean(stream_wide * stream_wide, axis=-1, keepdims=True) + epsilon)
        * norm_gain
    ).astype(jnp.bfloat16)
    token_count, top_count = routes.shape
    sequence_split = lax.axis_size("sp")
    device_count = sequence_split * core_split
    local_experts = expert_gate.shape[0]
    experts = local_experts * device_count
    capacity = 2 * token_count * top_count // experts
    flat_routes = routes.reshape(-1)
    onehot = (flat_routes[:, None] == jnp.arange(experts, dtype=jnp.int32)[None, :]).astype(
        jnp.int32
    )
    slot_index = jnp.sum(jnp.cumsum(onehot, axis=0) * onehot, axis=1) - 1
    target = flat_routes * capacity + slot_index
    source = (
        jnp.full((experts * capacity,), token_count, jnp.int32)
        .at[target]
        .set(jnp.arange(token_count * top_count, dtype=jnp.int32) // top_count)
    )
    padded_rows = jnp.concatenate([normed, jnp.zeros((1, model_width), normed.dtype)], axis=0)
    outgoing = padded_rows[source]
    shared_hidden = (
        jax.nn.silu(jnp.dot(normed, shared_gate, preferred_element_type=jnp.float32))
        * jnp.dot(normed, shared_up, preferred_element_type=jnp.float32)
    ).astype(jnp.bfloat16)
    shared_out = jnp.dot(shared_hidden, shared_down, preferred_element_type=jnp.float32)
    parcel = outgoing.reshape(device_count, local_experts, capacity, model_width)
    arrived = lax.all_to_all(parcel, ("sp", "tp"), split_axis=0, concat_axis=0, tiled=True)
    expert_rows = arrived[:, 0].reshape(-1, model_width)
    gate_part = jnp.dot(expert_rows, expert_gate[0], preferred_element_type=jnp.float32)
    up_part = jnp.dot(expert_rows, expert_up[0], preferred_element_type=jnp.float32)
    hidden = (jax.nn.silu(gate_part) * up_part).astype(jnp.bfloat16)
    result = jnp.dot(hidden, expert_down[0], preferred_element_type=jnp.float32).astype(
        jnp.bfloat16
    )
    results = [result.reshape(arrived.shape[0], arrived.shape[2], model_width)]
    returned = lax.all_to_all(
        jnp.stack(results, axis=1), ("sp", "tp"), split_axis=0, concat_axis=0, tiled=True
    )
    picked = returned.reshape(experts * capacity, model_width)[target].reshape(
        token_count, top_count, model_width
    )
    routed = jnp.zeros((token_count, model_width), jnp.float32)
    for route_index in range(top_count):
        routed = routed + route_weight[:, route_index, None] * picked[:, route_index].astype(
            jnp.float32
        )
    return (stream_wide + shared_out + routed).astype(jnp.bfloat16)


F32 = jnp.float32
BF16 = jnp.bfloat16
MESH_ID = pl.DeviceIdType.MESH
HALO = 32
CHUNK = 32
PLANES = 4
PARTS = 4
VMEM_LIMIT = 58 * 1024 * 1024


def flip(index, bits):
    out, weight = index, 1
    while weight <= bits:
        if (bits // weight) % 2:
            out = out + weight * (1 - 2 * ((index // weight) % 2))
        weight *= 2
    return out


def silu(v):
    return v / (1.0 + jnp.exp(-v))


ORDERS = {
    "E": (
        (
            "P00", "D01", "P02", "D03", "D00", "T10", "P03", "P01", "D02", "S00", "P11", "T20",
            "P10", "P13", "P12", "P21", "T30", "P20", "X01", "X10", "P22", "P23", "X00", "P30",
            "P33", "P31", "M10", "P32", "M12", "M11", "X20", "M13", "M03", "X30", "M20", "M02",
            "M22", "M01", "M23", "M30", "M31", "M32", "X31", "M33", "M21", "M00", "X21", "X11",
            "F02", "F01", "F00", "F03",
        ),
        (
            "S00", "T10", "D02", "P02", "P00", "T30", "P01", "P03", "X00", "D00", "D03", "D01",
            "X01", "X10", "X20", "T20", "P30", "P32", "M00", "X30", "P31", "P33", "P23", "P21",
            "P11", "P22", "P20", "X31", "P10", "P12", "P13", "M30", "M31", "X21", "M33", "M32",
            "M03", "M20", "M23", "M22", "M21", "X11", "M10", "M13", "M01", "M12", "M11", "M02",
            "F00", "F03", "F01", "F02",
        ),
    ),
    "I": (
        (
            "P03", "D00", "D10", "D11", "D01", "D02", "D13", "P01", "D03", "D12", "T10", "P00",
            "T20", "L21", "L20", "L11", "P11", "P20", "L22", "L13", "P02", "R00", "X01", "L10",
            "P21", "L12", "L23", "P22", "P10", "T30", "L31", "L33", "P31", "P23", "P13", "P33",
            "L30", "S00", "P12", "P30", "L32", "P32", "X00", "X10", "X20", "X30", "M00", "M20",
            "M22", "M23", "M01", "M30", "M31", "X31", "M32", "M03", "M02", "M33", "M10", "F03",
            "F00", "M11", "M21", "X11", "M12", "M13", "X21", "F02", "F01",
        ),
        (
            "P01", "P03", "T10", "T20", "P02", "P00", "R00", "X01", "L10", "L13", "L12", "M02",
            "T30", "X00", "M03", "L30", "D01", "D11", "L11", "P30", "L33", "D03", "D02", "P13",
            "L32", "P33", "P32", "P11", "D10", "P12", "L21", "L31", "X20", "L22", "D00", "L23",
            "P31", "D12", "P10", "X30", "S00", "L20", "P20", "D13", "P22", "P23", "M01", "X31",
            "P21", "X10", "X11", "X21", "M31", "M30", "M33", "M11", "M32", "M10", "M20", "M13",
            "M23", "M00", "M22", "M12", "M21", "F00", "F02", "F03", "F01",
        ),
    ),
}


def fused_kernel(n_sp, n_tp, capacity, *refs):
    hbm_in, out_ref = refs[:17], refs[17]
    vmem_in = refs[18:35]
    (
        glu_ext,
        ids_ext,
        tap_rows,
        halo_send,
        halo_recv,
        act,
        act_recv,
        ids_here,
        base_ref,
        mail,
        picks,
        highs,
        lows,
        tok,
        outgoing,
        arrived,
        result,
        returned,
        partial,
        inc,
        gate_acc,
        up_acc,
        hidden_ref,
        load_sem,
        halo_sem,
        act_sem,
        mail_send,
        mail_recv,
        tok_send,
        tok_recv,
        go_send,
        go_recv,
        back_send,
        back_recv,
        part_send,
        part_recv,
    ) = refs[35:]
    (
        value_ref,
        gate_ref,
        taps_ref,
        ids_ref,
        gain_ref,
        shift_ref,
        resid_ref,
        ngain_ref,
        routes_ref,
        weight_ref,
        conv_out,
        sg,
        su,
        sd,
        eg,
        eu,
        ed,
    ) = vmem_in
    n = n_sp * n_tp
    per = n // PLANES
    sp, tp = lax.axis_index("sp"), lax.axis_index("tp")
    me = sp * n_tp + tp
    plane, here = me // per, me % per
    rows, channels = value_ref.shape
    tokens, model = resid_ref.shape
    width = taps_ref.shape[0]
    group = glu_ext.shape[2]
    groups = channels // group
    cols = model // PARTS
    slots = per * capacity
    side = 1 - 2 * (plane // 2)
    edge = plane % (PLANES - 1) == 0
    inner = plane % (PLANES - 1) != 0
    inner_count = (plane % (PLANES - 1) + 1) // 2

    def place(index):
        return (index // n_tp, index % n_tp)

    inward = place((plane + side) * per + here)
    outward = place((plane - side) * per + here)
    peers = [flip(here, k) for k in range(per - 1, 0, -1)]

    def peer_place(peer):
        return place(plane * per + peer)

    loads = [
        pltpu.make_async_copy(a, b, load_sem.at[i])
        for i, (a, b) in enumerate(zip(hbm_in, vmem_in))
    ]
    barrier = pltpu.get_barrier_semaphore()

    def greet(where):
        pl.semaphore_signal(barrier, inc=1, device_id=where, device_id_type=MESH_ID)

    for load in loads:
        load.start()
    for peer in peers:
        greet(peer_place(peer))
    greet(inward)

    @pl.when(inner)
    def _():
        greet(outward)

    @pl.when(sp < n_sp - 1)
    def _():
        greet((sp + 1, tp))

    @pl.when(sp > 0)
    def _():
        greet((sp - 1, tp))

    has_next = 1 - (sp + 1) // n_sp
    has_last = (sp + n_sp - 1) // n_sp
    for load in loads[:10]:
        load.wait()

    mail[0, 0:2, :] = routes_ref[...].astype(F32)
    mail[0, 2:4, :] = weight_ref[...]
    glu = (value_ref[...].astype(F32) * jax.nn.sigmoid(gate_ref[...].astype(F32))).astype(BF16)
    halo_send[...] = glu[rows - HALO :, :]
    for g in range(groups):
        glu_ext[g, pl.ds(HALO, rows), :] = glu[:, g * group : (g + 1) * group].astype(F32)
    for at in range(0, rows, group):
        row = ids_ref[:, at : at + group].astype(F32)
        column = jnp.broadcast_to(row, (group, group)).T
        ids_here[pl.ds(at, group), :] = column
        ids_ext[pl.ds(HALO + at, group), :] = column
    tap_rows[pl.ds(0, width), :] = taps_ref[...].astype(F32)

    def remote(src, dst, send_sem, recv_sem, where):
        return pltpu.make_async_remote_copy(
            src_ref=src,
            dst_ref=dst,
            send_sem=send_sem,
            recv_sem=recv_sem,
            device_id=where,
            device_id_type=MESH_ID,
        )

    halo_copies = [
        remote(halo_send, halo_recv, halo_sem.at[0], halo_sem.at[1], (sp + 1, tp)),
        remote(
            ids_here.at[pl.ds(rows - HALO, HALO)],
            ids_ext.at[pl.ds(0, HALO)],
            halo_sem.at[2],
            halo_sem.at[3],
            (sp + 1, tp),
        ),
    ]

    @pl.when(sp == 0)
    def _():
        glu_ext[:, pl.ds(0, HALO), :] = jnp.zeros((groups, HALO, group), F32)
        ids_ext[pl.ds(0, HALO), :] = jnp.full((HALO, group), -1.0, F32)

    def mail_copy(sent, landed, index, where):
        return remote(
            mail.at[sent], mail.at[landed], mail_send.at[index], mail_recv.at[landed], where
        )

    mail_edge = mail_copy(0, 1, 0, inward)
    mail_in = mail_copy(0, 2, 0, inward)
    mail_out = mail_copy(0, 1, 1, outward)
    mail_relay = [
        mail_copy(1, 3, 2, inward),
        mail_copy(2, 2, 3, outward),
        mail_copy(3, 3, 4, outward),
    ]

    other = (tp + 1) % n_tp
    theirs = pl.multiple_of(other * tokens, tokens)
    mine_at = pl.multiple_of(tp * tokens, tokens)
    act_copy = remote(
        act.at[pl.ds(theirs, tokens)], act_recv, act_sem.at[0], act_sem.at[1], (sp, other)
    )
    lot = tokens // CHUNK
    late = lot + 2
    greeted = 2 * (1 - (plane + PLANES - 1) // PLANES)

    first = plane * per
    tri_r = lax.broadcasted_iota(jnp.int32, (tokens, tokens), 0)
    tri_c = lax.broadcasted_iota(jnp.int32, (tokens, tokens), 1)
    later = (tri_r < tri_c).astype(F32).astype(BF16)
    spread_t = (
        (
            lax.broadcasted_iota(jnp.int32, (slots, per), 0) // capacity
            == lax.broadcasted_iota(jnp.int32, (slots, per), 1)
        )
        .astype(F32)
        .astype(BF16)
    )
    row_slot = (lax.broadcasted_iota(jnp.int32, (slots, tokens), 0) % capacity).astype(F32)
    row_expert = (
        first + lax.broadcasted_iota(jnp.int32, (slots, tokens), 0) // capacity
    ).astype(F32)
    expert_row = (first + lax.broadcasted_iota(jnp.int32, (per, tokens), 0)).astype(F32)

    def tables(b):
        routes, weight = mail[b, 0:2, :], mail[b, 2:4, :]
        member = (
            (routes[0:1, :] == expert_row).astype(F32)
            + (routes[1:2, :] == expert_row).astype(F32)
        ).astype(BF16)
        slot = jnp.dot(member, later, preferred_element_type=F32).astype(BF16)
        right = jnp.dot(spread_t, slot, preferred_element_type=F32) == row_slot
        hit0 = jnp.where(right & (routes[0:1, :] == row_expert), 1.0, 0.0)
        hit1 = jnp.where(right & (routes[1:2, :] == row_expert), 1.0, 0.0)
        picks[b] = (hit0 + hit1).astype(BF16)
        mix = (hit0 * weight[0:1, :] + hit1 * weight[1:2, :]).T
        high = mix.astype(BF16)
        highs[b] = high
        lows[b] = (mix - high.astype(F32)).astype(BF16)

    def conv_step(i, carry):
        @pl.when(i == greeted)
        def _():
            pl.semaphore_wait(barrier, per - 1 + 1 + inner_count + has_next + has_last)

            @pl.when(sp < n_sp - 1)
            def _():
                for copy in halo_copies:
                    copy.start()

            @pl.when(edge)
            def _():
                mail_edge.start()

            @pl.when(inner)
            def _():
                mail_in.start()
                mail_out.start()

        @pl.when(i == late)
        def _():
            tables(0)

            @pl.when(sp > 0)
            def _():
                for copy in halo_copies:
                    copy.wait_recv()
                for g in range(groups):
                    glu_ext[g, pl.ds(0, HALO), :] = halo_recv[
                        :, g * group : (g + 1) * group
                    ].astype(F32)

        low = (
            (1 - i // lot) * (i + lot)
            + (i // lot) * (1 - i // late) * (i - lot + 1)
            + (i // (late + 1)) * (i - lot)
        )
        high = (1 - i // late) * (i + 1) + (i // (late + 1)) * i
        r = pl.multiple_of(((1 - tp) * low + tp * high) * CHUNK, CHUNK)
        mine = ids_here[pl.ds(r, CHUNK), :]
        sums = [jnp.zeros((CHUNK, group), F32) for _ in range(groups)]
        for tap in range(width):
            off = HALO - width + 1 + tap
            same = ids_ext[pl.ds(r + off, CHUNK), :] == mine
            for g in range(groups):
                term = (
                    tap_rows[tap : tap + 1, g * group : (g + 1) * group]
                    * glu_ext[g, pl.ds(r + off, CHUNK), :]
                )
                sums[g] = sums[g] + jnp.where(same, term, 0.0)
        for g in range(groups):
            at = slice(g * group, (g + 1) * group)
            centered = sums[g] - jnp.mean(sums[g], axis=-1, keepdims=True)
            var = jnp.mean(centered * centered, axis=-1, keepdims=True)
            v = centered * lax.rsqrt(var + epsilon) * gain_ref[:, at] + shift_ref[:, at]
            act[pl.ds(r, CHUNK), at] = silu(v).astype(BF16)

        @pl.when((i == lot - 1) & (tp == 0))
        def _():
            act_copy.start()

        @pl.when((i == late) & (tp == 1))
        def _():
            act_copy.start()

        return carry

    lax.fori_loop(0, rows // CHUNK, conv_step, 0)

    @pl.when(inner)
    def _():
        mail_copy(1, 1, 0, inward).wait_recv()
        mail_relay[0].start()
        mail_copy(2, 2, 0, inward).wait_recv()
        mail_relay[1].start()

    loads[10].wait()
    projected = jnp.dot(
        act[pl.ds(mine_at, tokens), :],
        conv_out[pl.ds(pl.multiple_of(tp * channels, channels), channels), :],
        preferred_element_type=F32,
    )
    act_copy.wait_recv()
    projected = projected + jnp.dot(
        act_recv[...],
        conv_out[pl.ds(pl.multiple_of(other * channels, channels), channels), :],
        preferred_element_type=F32,
    )
    stream = (resid_ref[...].astype(F32) + projected).astype(BF16).astype(F32)
    normed = (
        stream
        * lax.rsqrt(jnp.mean(stream * stream, axis=-1, keepdims=True) + epsilon)
        * ngain_ref[...]
    ).astype(BF16)
    for q in range(PARTS):
        tok[0, q] = normed[:, q * cols : (q + 1) * cols]
        base_ref[q] = stream[:, q * cols : (q + 1) * cols]

    def piece(index):
        return pl.ds(pl.multiple_of(index * capacity, capacity), capacity)

    chips = per // n_tp
    lane = chips * capacity
    chip = here // n_tp
    mine_row = tp * chips + chip

    def toward(sign):
        return place((plane + side * sign) * per + here)

    def tok_copy(sent, landed, index, q, where):
        return remote(
            tok.at[sent, q], tok.at[landed, q], tok_send.at[index, q], tok_recv.at[landed, q], where
        )

    def part_copy(b, landed, q, where):
        return remote(
            partial.at[b, q], inc.at[landed, q], part_send.at[b, q], part_recv.at[landed, q], where
        )

    def bytes_of(buffer, b, q, count, sem):
        area = buffer.at[b, q, pl.ds(0, count * capacity)]
        return remote(area, area, sem, sem, inward)

    def send_rows(core, b, q):
        for peer in peers:
            remote(
                outgoing.at[b, q, piece(peer)],
                arrived.at[b, q, piece(mine_row)],
                go_send.at[b, q],
                go_recv.at[b, q, core],
                peer_place(peer),
            ).start()
        arrived[b, q, piece(mine_row), :] = outgoing[b, q, piece(here), :]

    def return_rows(core, b, q, s):
        for apart in range(chips - 1, -1, -1):
            target = flip(chip, apart)
            if apart == 0 and s == core:
                returned[b, q, piece(here), :] = result[b, q, piece(mine_row), :]
            else:
                remote(
                    result.at[b, q, piece(s * chips + target)],
                    returned.at[b, q, piece(here)],
                    back_send.at[b, q],
                    back_recv.at[b, q],
                    peer_place(target * n_tp + s),
                ).start()

    landing = {"E": {0: (1, 1)}, "I": {0: (2, 1), 1: (1, -1)}}
    relaying = {1: (3, 2, 1), 2: (2, 3, -1), 3: (3, 4, -1)}
    part_to = {
        "E": {1: (0, 1), 2: (2, 1), 3: (3, 1)},
        "I": {1: (0, -1), 2: (1, 1), 3: (4, 1)},
    }
    joins = {1: 4, 2: 2, 3: 3}
    closes = {"E": (0,), "I": (0, 1)}

    def op(role, core, kind, b, q):
        if kind == "D":
            landed, sign = landing[role][b]
            tok_copy(0, landed, b, q, toward(sign)).start()
        elif kind == "T":
            if role == "E":
                mail_copy(b, b, 0, inward).wait_recv()
            tables(b)
        elif kind == "R":
            mail_copy(3, 3, 0, inward).wait_recv()
            mail_relay[2].start()
        elif kind == "L":
            tok_copy(b, b, 0, q, inward).wait_recv()
            landed, index, sign = relaying[b]
            tok_copy(b, landed, index, q, toward(sign)).start()
        elif kind == "P":
            if role == "E" and b:
                tok_copy(b, b, 0, q, inward).wait_recv()
            outgoing[b, q] = jnp.dot(picks[b], tok[b, q], preferred_element_type=F32).astype(BF16)
            send_rows(core, b, q)
        elif kind == "S":
            gate = jnp.zeros((tokens, sg.shape[1]), F32)
            up = jnp.zeros((tokens, sg.shape[1]), F32)
            for p in range(PARTS):
                k = slice(p * cols, (p + 1) * cols)
                gate = gate + jnp.dot(tok[0, p], sg[k, :], preferred_element_type=F32)
                up = up + jnp.dot(tok[0, p], su[k, :], preferred_element_type=F32)
            hidden = (silu(gate) * up).astype(BF16)
            for p in range(PARTS):
                k = slice(p * cols, (p + 1) * cols)
                base_ref[p] += jnp.dot(hidden, sd[:, k], preferred_element_type=F32)
        elif kind == "X":
            s, at = q, slice(q * lane, (q + 1) * lane)
            count = chips - int(s == core)
            gate_acc[...] = jnp.zeros((lane, eg.shape[2]), F32)
            up_acc[...] = jnp.zeros((lane, eg.shape[2]), F32)

            def widen(p, carry):
                k = pl.ds(pl.multiple_of(p * cols, cols), cols)
                bytes_of(arrived, b, p, count, go_recv.at[b, p, s]).wait_recv()
                x = arrived[b, p, at, :]
                gate_acc[...] += jnp.dot(x, eg[0, k, :], preferred_element_type=F32)
                up_acc[...] += jnp.dot(x, eu[0, k, :], preferred_element_type=F32)
                return carry

            lax.fori_loop(0, PARTS, widen, 0, unroll=2)
            hidden_ref[...] = (silu(gate_acc[...]) * up_acc[...]).astype(BF16)

            def narrow(p, carry):
                k = pl.ds(pl.multiple_of(p * cols, cols), cols)
                result[b, p, at, :] = jnp.dot(
                    hidden_ref[...], ed[0, :, k], preferred_element_type=F32
                ).astype(BF16)
                return_rows(core, b, p, s)
                return carry

            lax.fori_loop(0, PARTS, narrow, 0, unroll=2)
        elif kind == "M":
            bytes_of(returned, b, q, per - 1, back_recv.at[b, q]).wait_recv()
            back = returned[b, q]
            mixed = jnp.dot(highs[b], back, preferred_element_type=F32) + jnp.dot(
                lows[b], back, preferred_element_type=F32
            )
            if b == 0:
                base_ref[q] += mixed
                return
            if role == "I":
                joined = joins[b]
                part_copy(b, joined, q, inward).wait_recv()
                mixed = mixed + inc[joined, q].astype(F32)
            partial[b, q] = mixed.astype(BF16)
            landed, sign = part_to[role][b]
            part_copy(b, landed, q, toward(sign)).start()
        elif kind == "F":
            total = base_ref[q]
            for joined in closes[role]:
                part_copy(1, joined, q, inward).wait_recv()
                total = total + inc[joined, q].astype(F32)
            out_ref[:, q * cols : (q + 1) * cols] = total.astype(BF16)

    def close(role):
        for index, (landed, sign) in landing[role].items():
            for q in range(PARTS):
                tok_copy(0, landed, index, q, toward(sign)).wait_send()
        for b, (landed, index, sign) in relaying.items():
            if role == "I":
                for q in range(PARTS):
                    tok_copy(b, landed, index, q, toward(sign)).wait_send()
        for b, (landed, sign) in part_to[role].items():
            for q in range(PARTS):
                part_copy(b, landed, q, toward(sign)).wait_send()

    for load in loads[11:]:
        load.wait()
    for core in range(n_tp):
        for role, chosen in (("E", edge), ("I", inner)):

            @pl.when(chosen & (tp == core))
            def _(role=role, core=core):
                for step in ORDERS[role][core]:
                    op(role, core, step[0], int(step[1]), int(step[2]))
                close(role)

    @pl.when(edge)
    def _():
        mail_edge.wait_send()

    @pl.when(inner)
    def _():
        mail_in.wait_send()
        mail_out.wait_send()
        for copy in mail_relay:
            copy.wait_send()

    act_copy.wait_send()

    @pl.when(sp < n_sp - 1)
    def _():
        for copy in halo_copies:
            copy.wait_send()

    for b in range(PLANES):
        for q in range(PARTS):
            bytes_of(outgoing, b, q, per - 1, go_send.at[b, q]).wait_send()
            bytes_of(result, b, q, per - 1, back_send.at[b, q]).wait_send()


def fused(
    conv_value,
    conv_gate,
    taps,
    doc_ids,
    gn_gain,
    gn_shift,
    conv_out,
    residual,
    norm_gain,
    routes,
    route_weight,
    expert_gate,
    expert_up,
    expert_down,
    shared_gate,
    shared_up,
    shared_down,
):
    n_sp, n_tp = lax.axis_size("sp"), lax.axis_size("tp")
    n = n_sp * n_tp
    rows, channels = conv_value.shape
    tokens, model = residual.shape
    capacity = 2 * tokens * routes.shape[1] // n
    group = channels * n_tp // GROUPS
    slots = n // PLANES * capacity
    cols = model // PARTS
    operands = (
        conv_value,
        conv_gate,
        taps,
        doc_ids[None, :],
        gn_gain[None, :],
        gn_shift[None, :],
        residual,
        norm_gain[None, :],
        routes.T,
        route_weight.T,
        conv_out,
        shared_gate,
        shared_up,
        shared_down,
        expert_gate,
        expert_up,
        expert_down,
    )
    hbm = pl.BlockSpec(memory_space=pl.ANY)
    dma = pltpu.SemaphoreType.DMA
    return pl.pallas_call(
        functools.partial(fused_kernel, n_sp, n_tp, capacity),
        out_shape=pltpu.VMEM((tokens, model), BF16),
        in_specs=[hbm] * len(operands),
        out_specs=pl.BlockSpec(memory_space=pltpu.VMEM),
        scratch_shapes=[pltpu.VMEM(x.shape, x.dtype) for x in operands]
        + [
            pltpu.VMEM((channels // group, rows + HALO, group), F32),
            pltpu.VMEM((rows + HALO, group), F32),
            pltpu.VMEM((taps.shape[0] + 1, channels), F32),
            pltpu.VMEM((HALO, channels), BF16),
            pltpu.VMEM((HALO, channels), BF16),
            pltpu.VMEM((rows, channels), BF16),
            pltpu.VMEM((tokens, channels), BF16),
            pltpu.VMEM((rows, group), F32),
            pltpu.VMEM((PARTS, tokens, cols), F32),
            pltpu.VMEM((PLANES, 4, tokens), F32),
            pltpu.VMEM((PLANES, slots, tokens), BF16),
            pltpu.VMEM((PLANES, tokens, slots), BF16),
            pltpu.VMEM((PLANES, tokens, slots), BF16),
            pltpu.VMEM((PLANES, PARTS, tokens, cols), BF16),
            pltpu.VMEM((PLANES, PARTS, slots, cols), BF16),
            pltpu.VMEM((PLANES, PARTS, slots, cols), BF16),
            pltpu.VMEM((PLANES, PARTS, slots, cols), BF16),
            pltpu.VMEM((PLANES, PARTS, slots, cols), BF16),
            pltpu.VMEM((PLANES, PARTS, tokens, cols), BF16),
            pltpu.VMEM((5, PARTS, tokens, cols), BF16),
            pltpu.VMEM((slots // n_tp, expert_gate.shape[2]), F32),
            pltpu.VMEM((slots // n_tp, expert_gate.shape[2]), F32),
            pltpu.VMEM((slots // n_tp, expert_gate.shape[2]), BF16),
            dma((17,)),
            dma((4,)),
            dma((2,)),
            dma((5,)),
            dma((PLANES,)),
            dma((5, PARTS)),
            dma((PLANES, PARTS)),
            dma((PLANES, PARTS)),
            dma((PLANES, PARTS, n_tp)),
            dma((PLANES, PARTS)),
            dma((PLANES, PARTS)),
            dma((PLANES, PARTS)),
            dma((5, PARTS)),
        ],
        compiler_params=pltpu.CompilerParams(
            collective_id=0, has_side_effects=True, vmem_limit_bytes=VMEM_LIMIT
        ),
    )(*operands)


def fits(mesh):
    n = mesh.size
    return n & (n - 1) == 0 and 8 < n <= 32 and mesh.shape["tp"] == 2


def solution(mesh):
    return jax.shard_map(
        fused if fits(mesh) else per_device,
        mesh=mesh,
        in_specs=(
            P("sp", "tp"),
            P("sp", "tp"),
            P(None, "tp"),
            P("sp"),
            P("tp"),
            P("tp"),
            P(),
            P(("sp", "tp"), None),
            P(),
            P(("sp", "tp"), None),
            P(("sp", "tp"), None),
            P(("sp", "tp"), None, None),
            P(("sp", "tp"), None, None),
            P(("sp", "tp"), None, None),
            P(),
            P(),
            P(),
        ),
        out_specs=P(("sp", "tp"), None),
        check_vma=False,
    )
```
